128 devices in a mesh: rep: 2 (over x_hi), fs: 16 (over y, x_lo, core), tp: 4 (over z).
Axes of the slice: x: 4 (x_hi: 2, x_lo: 2; x = x_hi * 2 + x_lo), y: 4, z: 4, core: 2. Of those that a mesh axis runs over, the one named last changes fastest.
Arguments:
- tokens: bfloat16 [16384, 2048], P(('rep', 'fs', 'tp')), may hold values from -3 to 3
- mixer_output: bfloat16 [16384, 2048], P(('rep', 'fs', 'tp')), may hold values from -6 to 6
- early_norm: float32 [2048], replicated, may hold values from 0.75 to 1.25
- early_gate: bfloat16 [2048, 5120], P('fs', 'tp'), may hold values from -0.125 to 0.125
- early_value: bfloat16 [2048, 5120], P('fs', 'tp'), may hold values from -0.125 to 0.125
- early_down: bfloat16 [5120, 2048], P('tp', 'fs'), may hold values from -0.078125 to 0.078125
- early_post: float32 [2048], replicated, may hold values from 0.75 to 1.25
- mixer_gain: float32 [2048], replicated, may hold values from 0.75 to 1.25
- later_norm: float32 [2048], replicated, may hold values from 0.75 to 1.25
- later_gate: bfloat16 [2048, 5120], P('fs', 'tp'), may hold values from -0.125 to 0.125
- later_value: bfloat16 [2048, 5120], P('fs', 'tp'), may hold values from -0.125 to 0.125
- later_down: bfloat16 [5120, 2048], P('tp', 'fs'), may hold values from -0.078125 to 0.078125
- later_post: float32 [2048], replicated, may hold values from 0.75 to 1.25
Outputs:
- layer_out: bfloat16 [16384, 2048], P(('rep', 'fs', 'tp'))
The draws below stay inside these ranges and needn't reach their ends.
All inputs are finite; a program needn't handle non-finite values.
Results may differ from the reference program's by a relative error of at most 0.015.
Values may be sent and summed in bfloat16 or wider, within the bound.
A program may use at most 128 MiB of HBM per device.

```python
import jax
import jax.numpy as jnp
from jax import lax

D = 2048
FF = 5120
TOKENS = 16384


def steps_of(rng, extent, split, low, top_value):
    def one(position, parts):
        draws = jax.random.uniform(jax.random.fold_in(jax.random.fold_in(rng, 6), position), (parts,), jnp.float32, low / len(split), top_value / len(split))
        return jnp.repeat(jnp.exp(draws), extent[position] // parts).reshape((-1,) + (1,) * (len(extent) - position - 1))

    loudness = one(*split[0])
    for cut in split[1:]:
        loudness = loudness * one(*cut)
    return loudness


def scatter_about(stream_key, dims, scale, bound, cuts=(), dtype=jnp.bfloat16):
    array = jax.random.normal(stream_key, dims, jnp.float32) * scale
    if len(cuts) > 0:
        array = steps_of(stream_key, dims, cuts, -0.22, 0.18) * array
    return jnp.clip(array, min=-bound, max=bound).astype(dtype)


def setup_inputs(seed: int = 0) -> dict:
    keys = jax.random.split(jax.random.key(seed), 14)
    return {
        "tokens": scatter_about(keys[0], (TOKENS, D), 0.5, 3.0, ((0, 128),)),
        "mixer_output": scatter_about(keys[1], (TOKENS, D), 1.0, 6.0, ((0, 128),)),
        "early_norm": jnp.clip(1.0 + 0.05 * jax.random.normal(keys[2], (D,), jnp.float32), 0.75, 1.25),
        "early_gate": scatter_about(keys[3], (D, FF), D ** -0.5, 0.125, ((0, 16), (1, 4))),
        "early_value": scatter_about(keys[4], (D, FF), D ** -0.5, 0.125, ((0, 16), (1, 4))),
        "early_down": scatter_about(keys[5], (FF, D), FF ** -0.5, 0.078125, ((0, 4), (1, 16))),
        "early_post": jnp.clip(1.0 + 0.05 * jax.random.normal(keys[6], (D,), jnp.float32), 0.75, 1.25),
        "mixer_gain": jnp.clip(1.0 + 0.05 * jax.random.normal(keys[7], (D,), jnp.float32), 0.75, 1.25),
        "later_norm": jnp.clip(1.0 + 0.05 * jax.random.normal(keys[8], (D,), jnp.float32), 0.75, 1.25),
        "later_gate": scatter_about(keys[9], (D, FF), D ** -0.5, 0.125, ((0, 16), (1, 4))),
        "later_value": scatter_about(keys[10], (D, FF), D ** -0.5, 0.125, ((0, 16), (1, 4))),
        "later_down": scatter_about(keys[11], (FF, D), FF ** -0.5, 0.078125, ((0, 4), (1, 16))),
        "later_post": jnp.clip(1.0 + 0.05 * jax.random.normal(keys[12], (D,), jnp.float32), 0.75, 1.25),
    }


epsilon = 1e-06

def rms_scale(values, gain):
    values = values.astype(jnp.float32)
    scale = lax.rsqrt(lax.optimization_barrier(jnp.mean(values * values, axis=-1, keepdims=True)) + epsilon)
    return values * scale * gain

def half_branch(normed, w_gate, w_value, w_down):
    gate_sum = jnp.dot(normed, w_gate, preferred_element_type=jnp.float32)
    value_sum = jnp.dot(normed, w_value, preferred_element_type=jnp.float32)
    hidden = (jax.nn.silu(gate_sum) * value_sum).astype(jnp.bfloat16)
    return jnp.dot(hidden, w_down, preferred_element_type=jnp.float32)

def reference(tokens, mixer_output, early_norm, early_gate, early_value, early_down, early_post, mixer_gain, later_norm, later_gate, later_value, later_down, later_post):
    early_in = rms_scale(tokens, early_norm).astype(jnp.bfloat16)
    early_branch = half_branch(early_in, early_gate, early_value, early_down)
    mixed = tokens.astype(jnp.float32) + 0.5 * rms_scale(early_branch, early_post) + rms_scale(mixer_output, mixer_gain)
    mixed = mixed.astype(jnp.bfloat16)
    later_in = rms_scale(mixed, later_norm).astype(jnp.bfloat16)
    later_branch = half_branch(later_in, later_gate, later_value, later_down)
    layer_out = mixed.astype(jnp.float32) + 0.5 * rms_scale(later_branch, later_post)
    return layer_out.astype(jnp.bfloat16)
```

```python
import functools

import jax
import jax.numpy as jnp
from jax import lax
from jax.experimental import pallas as pl
from jax.experimental.pallas import tpu as pltpu
from jax.sharding import PartitionSpec as P

epsilon = 1e-06
GROUPS = ((0, 0), (1, 0), (3, 0), (0, 1), (2, 0), (3, 1), (1, 1), (2, 1))
TILE = 256
Y, X, T = 4, 4, 4

PIECES = {
    "ypA": (3, 0, 0, 2), "ypB": (3, 0, 2, 2), "ymA": (1, 0, 0, 2), "ymB": (1, 0, 2, 2),
    "fA": (2, 0, 0, 2), "fB": (2, 0, 2, 2),
    "xA": (0, 1, 0, 2), "xB": (0, 1, 2, 2),
    "qp": (3, 1, 0, 1), "qm": (1, 1, 2, 1),
    "x1a": (3, 1, 1, 1), "x1b": (3, 1, 2, 2), "x2a": (1, 1, 0, 2), "x2b": (1, 1, 3, 1),
    "x3a": (2, 1, 0, 2), "x3b": (2, 1, 2, 2),
}
ROUTES = {
    "ypA": ("y+", None), "ypB": ("y+", None), "ymA": ("y-", None), "ymB": ("y-", None),
    "xA": ("x+", None), "xB": ("x-", None),
    "fA": ("y+", "ypA"), "fB": ("y-", "ymB"),
    "qp": ("y+", "xA"), "qm": ("y-", "xB"),
    "x1a": ("x+", "ypA"), "x1b": ("x-", "ypB"), "x2a": ("x+", "ymA"), "x2b": ("x-", "ymB"),
    "x3a": ("x+", "fA"), "x3b": ("x-", "fB"),
}


def rms_scale(values, gain):
    scale = lax.rsqrt(jnp.mean(values * values, axis=-1, keepdims=True) + epsilon)
    return values * scale * gain


def kernel(
    tokens, mixer, early_norm, w0, w1, w2, early_post, mixer_gain, later_norm, w3, w4, w5, later_post,
    out,
    g0, g1, g2, g3, g4, g5, rows0, rows1, gate_sum, hidden, part, base, branch, mixed, from_far, from_short, from_long,
    w_send, w_recv, local_sem, z_send, z_recv,
):
    source = (w0, w1, w2, w3, w4, w5)
    full = (g0, g1, g2, g3, g4, g5)
    all_rows = (rows0, rows1)
    r, f, t = lax.axis_index("rep"), lax.axis_index("fs"), lax.axis_index("tp")
    c = f % 2
    xl = f // 2 % 2
    y = f // 4
    x = r * 2 + xl
    n, D = tokens.shape

    def chip(dx, dy):
        xx = (x + dx) % X
        return {"rep": xx // 2, "fs": ((y + dy) % Y * 2 + xx % 2) * 2 + c}

    where = {"y+": chip(0, 1), "y-": chip(0, Y - 1), "x+": chip(1, 0), "x-": chip(X - 1, 0)}
    mate = {"fs": f + 1 - 2 * c}
    z_right, z_left = {"tp": (t + 1) % T}, {"tp": (t + T - 1) % T}

    barrier = pltpu.get_barrier_semaphore()
    partners = [mate, *where.values(), z_right, z_left]
    for who in partners:
        pl.semaphore_signal(barrier, inc=1, device_id=who, device_id_type=pl.DeviceIdType.MESH)
    pl.semaphore_wait(barrier, len(partners))

    pending = []
    copies = {}
    counts = {"w": 0, "z": 0}

    def send(kind, key, src, dst, who):
        index = counts[kind]
        counts[kind] += 1
        sems = (w_send, w_recv) if kind == "w" else (z_send, z_recv)
        copy = pltpu.make_async_remote_copy(
            src_ref=src, dst_ref=dst, send_sem=sems[0].at[index], recv_sem=sems[1].at[index],
            device_id=who, device_id_type=pl.DeviceIdType.MESH,
        )
        copy.start()
        pending.append(copy)
        copies[key] = copy

    def owner(dy, other, core):
        return ((y + dy) % Y * 2 + (xl + other) % 2) * 2 + core

    def piece(m, shard, first, quarters):
        quarter = source[m].shape[0] // 4
        if m % 3 == 2:
            return full[m].at[shard, pl.ds(first * quarter, quarters * quarter)]
        start = pl.multiple_of(shard * 4 * quarter + first * quarter, quarter)
        return full[m].at[pl.ds(start, quarters * quarter)]

    def own_piece(m, name):
        quarter = source[m].shape[0] // 4
        _, _, first, quarters = PIECES[name]
        return source[m].at[pl.ds(first * quarter, quarters * quarter)]

    def pass_on(m, name):
        way, have = ROUTES[name]
        _, _, first, quarters = PIECES[name]
        if have is None:
            send("w", (name, m), own_piece(m, name), piece(m, f, first, quarters), where[way])
        else:
            dy, other, _, _ = PIECES[have]
            ref = piece(m, owner(dy, other, c), first, quarters)
            send("w", (name, m), ref, ref, where[way])

    def take(m, name, *onward):
        copies[name, m].wait_recv()
        for other in onward:
            pass_on(m, other)
        dy, column, first, quarters = PIECES[name]
        ref = piece(m, owner(dy, column, c), first, quarters)
        send("w", ("mate", name, m), ref, ref, mate)

    def own_y(m):
        for name in ("ypA", "ymB", "ypB", "ymA"):
            pass_on(m, name)

    def own_x(m):
        pass_on(m, "xA")
        pass_on(m, "xB")

    def own_mate(m):
        send("w", ("mate", "own", m), source[m], piece(m, f, 0, 4), mate)
        local = pltpu.make_async_copy(source[m], piece(m, f, 0, 4), local_sem.at[m])
        local.start()
        copies["local", m] = local

    def p1(m):
        take(m, "ypA", "fA", "x1a")
        take(m, "ymB", "fB", "x2b")

    def p2(m):
        take(m, "xA", "qp")
        take(m, "xB", "qm")

    def p3(m):
        take(m, "ypB", "x1b")
        take(m, "ymA", "x2a")

    def p4(m):
        take(m, "fA", "x3a")
        take(m, "fB", "x3b")

    def p5(m):
        for name in ("x1a", "x2b", "qp", "qm", "x1b", "x2a", "x3a", "x3b"):
            take(m, name)

    def ready(m, *groups):
        for dy, other in groups or GROUPS:
            if (dy, other) == (0, 0):
                copies["local", m].wait()
                copies["mate", "own", m].wait_recv()
            for name, (py, px, _, _) in PIECES.items():
                if (py, px) == (dy, other):
                    copies["mate", name, m].wait_recv()

    H = n // 2

    def row_half(ref, block, half):
        return ref.at[pl.ds(pl.multiple_of(block * n + half * H, H), H)]

    def gather_own(layer, half):
        ref = row_half(all_rows[layer], t, half)
        send("z", ("ag", layer, "r", half), ref, ref, z_right)
        send("z", ("ag", layer, "l", half), ref, ref, z_left)

    def gather_relay(layer):
        copies["ag", layer, "r", 0].wait_recv()
        ref = row_half(all_rows[layer], (t + T - 1) % T, 0)
        send("z", ("far", layer, 0), ref, ref, z_right)
        copies["ag", layer, "l", 1].wait_recv()
        ref = row_half(all_rows[layer], (t + 1) % T, 1)
        send("z", ("far", layer, 1), ref, ref, z_left)

    def gather_near(layer):
        copies["ag", layer, "r", 1].wait_recv()
        copies["ag", layer, "l", 0].wait_recv()

    def gather_far(layer):
        copies["far", layer, 0].wait_recv()
        copies["far", layer, 1].wait_recv()

    def gate(layer, first, last):
        weight = full[3 * layer]

        @pl.loop(first, last)
        def _(j):
            at = pl.ds(pl.multiple_of(j * TILE, TILE), TILE)
            gate_sum[:, at] = jnp.dot(all_rows[layer][...], weight[:, at], preferred_element_type=jnp.float32)

    def value(layer, first, last):
        weight = full[3 * layer + 1]

        @pl.loop(first, last)
        def _(j):
            at = pl.ds(pl.multiple_of(j * TILE, TILE), TILE)
            b = jnp.dot(all_rows[layer][...], weight[:, at], preferred_element_type=jnp.float32)
            a = gate_sum[:, at]
            hidden[:, at] = (a / (1.0 + jnp.exp(-a)) * b).astype(jnp.bfloat16)

    def block(layer, j, b):
        return part.at[layer, j, pl.ds(pl.multiple_of(b * n, n), n)]

    def down(layer, j):
        weight = full[3 * layer + 2]
        dy, other = GROUPS[j]
        both = jnp.concatenate([weight[owner(dy, other, 0)], weight[owner(dy, other, 1)]], axis=1)
        sums = jnp.dot(hidden[...], both, preferred_element_type=jnp.float32)
        part[layer, j] = sums.astype(jnp.bfloat16)
        long, short = (z_right, z_left) if j % 2 == 0 else (z_left, z_right)
        near = (t + T - 1) % T if j % 2 == 0 else (t + 1) % T
        send("z", ("rs2", layer, j), block(layer, j, (t + 2) % T), from_far.at[layer, j], long)
        send("z", ("rss", layer, j), block(layer, j, near), from_short.at[layer, j], short)

    def sum_step(layer, j):
        copies["rs2", layer, j].wait_recv()
        long, near = (z_right, (t + 1) % T) if j % 2 == 0 else (z_left, (t + T - 1) % T)
        mine = block(layer, j, near)
        mine[...] = (mine[...].astype(jnp.float32) + from_far[layer, j].astype(jnp.float32)).astype(jnp.bfloat16)
        send("z", ("rsl", layer, j), mine, from_long.at[layer, j], long)

    def sum_own(layer, j):
        copies["rss", layer, j].wait_recv()
        copies["rsl", layer, j].wait_recv()
        dy, other = GROUPS[j]
        at = pl.ds(pl.multiple_of(owner(dy, other, 0) * (D // 16), 2 * D // 16), 2 * D // 16)
        branch[:, at] = (
            block(layer, j, t)[...].astype(jnp.float32)
            + from_short[layer, j].astype(jnp.float32)
            + from_long[layer, j].astype(jnp.float32)
        )

    def finish_early(half):
        rows = pl.ds(half * H, H)
        keep = (base[rows] + 0.5 * rms_scale(branch[rows], early_post[...])).astype(jnp.bfloat16)
        mixed[rows] = keep
        row_half(rows1, t, half)[...] = rms_scale(keep.astype(jnp.float32), later_norm[...]).astype(jnp.bfloat16)
        gather_own(1, half)

    tiles = hidden.shape[1] // TILE

    own_y(0)
    own_x(0)
    own_x(1)
    own_mate(0)
    own_mate(1)
    for half in range(2):
        rows = pl.ds(half * H, H)
        row_half(rows0, t, half)[...] = rms_scale(tokens[rows].astype(jnp.float32), early_norm[...]).astype(jnp.bfloat16)
        gather_own(0, half)
    p1(0)
    p2(0)
    own_y(1)
    gather_relay(0)
    p3(0)
    own_x(2)
    own_mate(2)
    p4(0)
    base[...] = tokens[...].astype(jnp.float32) + rms_scale(mixer[...].astype(jnp.float32), mixer_gain[...])
    gather_near(0)
    p1(1)
    p2(1)
    own_y(2)
    p5(0)
    gather_far(0)
    ready(0)
    gate(0, 0, 2)
    p3(1)
    own_x(3)
    own_mate(3)
    gate(0, 2, tiles)
    p4(1)
    p1(2)
    p2(2)
    own_y(3)
    p5(1)
    ready(1)
    value(0, 0, 2)
    p3(2)
    own_x(4)
    own_mate(4)
    value(0, 2, tiles)
    ready(2, *GROUPS[:4])
    down(0, 0)
    down(0, 1)
    p4(2)
    down(0, 2)
    down(0, 3)
    sum_step(0, 0)
    sum_step(0, 1)
    ready(2, GROUPS[4])
    down(0, 4)
    p1(3)
    p2(3)
    own_y(4)
    sum_step(0, 2)
    sum_step(0, 3)
    p5(2)
    ready(2, *GROUPS[5:])
    down(0, 5)
    p3(3)
    own_x(5)
    own_mate(5)
    down(0, 6)
    down(0, 7)
    sum_step(0, 4)
    for j in range(4):
        sum_own(0, j)
    p4(3)
    for j in range(5, 8):
        sum_step(0, j)
    for j in range(4, 8):
        sum_own(0, j)
    finish_early(0)
    finish_early(1)
    p1(4)
    p2(4)
    own_y(5)
    p5(3)
    p3(4)
    p4(4)
    gather_relay(1)
    ready(3)
    gather_near(1)
    p1(5)
    p2(5)
    p5(4)
    ready(4)
    p3(5)
    gather_far(1)
    gate(1, 0, tiles)
    p4(5)
    value(1, 0, tiles)
    ready(5, *GROUPS[:5])
    for j in range(4):
        down(1, j)
    p5(5)
    sum_step(1, 0)
    sum_step(1, 1)
    down(1, 4)
    ready(5, *GROUPS[5:])
    down(1, 5)
    sum_step(1, 2)
    sum_step(1, 3)
    down(1, 6)
    down(1, 7)
    for j in range(4):
        sum_step(1, 4 + j)
        sum_own(1, j)
    for j in range(4, 8):
        sum_own(1, j)
    out[...] = (
        mixed[...].astype(jnp.float32) + 0.5 * rms_scale(branch[...], later_post[...])
    ).astype(jnp.bfloat16)
    for copy in pending:
        copy.wait_send()


def on_device(*args):
    (tokens, mixer, early_norm, eg, ev, ed, early_post, mixer_gain, later_norm, lg, lv, ld, later_post) = args
    n, D = tokens.shape
    depth, wide = eg.shape
    F = D // depth
    bf16, f32 = jnp.bfloat16, jnp.float32
    gains = [x.reshape(1, D) for x in (early_norm, early_post, mixer_gain, later_norm, later_post)]
    vmem = pl.BlockSpec(memory_space=pltpu.VMEM)
    hbm = pl.BlockSpec(memory_space=pl.ANY)
    gathered = [pltpu.VMEM((F * depth, wide), bf16)] * 2 + [pltpu.VMEM((F,) + ed.shape, bf16)]
    w_count = 6 * (2 * len(PIECES) + 1)
    z_count = 2 * (6 + 3 * len(GROUPS))
    landing = pltpu.VMEM((2, len(GROUPS), n, TILE), bf16)
    return pl.pallas_call(
        kernel,
        out_shape=jax.ShapeDtypeStruct((n, D), bf16),
        in_specs=[vmem] * 3 + [hbm] * 3 + [vmem] * 3 + [hbm] * 3 + [vmem],
        out_specs=vmem,
        scratch_shapes=gathered * 2
        + [
            pltpu.VMEM((T * n, D), bf16),
            pltpu.VMEM((T * n, D), bf16),
            pltpu.VMEM((T * n, wide), f32),
            pltpu.VMEM((T * n, wide), bf16),
            pltpu.VMEM((2, len(GROUPS), T * n, TILE), bf16),
            pltpu.VMEM((n, D), f32),
            pltpu.VMEM((n, D), f32),
            pltpu.VMEM((n, D), bf16),
            landing,
            landing,
            landing,
            pltpu.SemaphoreType.DMA((w_count,)),
            pltpu.SemaphoreType.DMA((w_count,)),
            pltpu.SemaphoreType.DMA((6,)),
            pltpu.SemaphoreType.DMA((z_count,)),
            pltpu.SemaphoreType.DMA((z_count,)),
        ],
        compiler_params=pltpu.CompilerParams(
            collective_id=0, has_side_effects=True, vmem_limit_bytes=66_000_000
        ),
    )(tokens, mixer, gains[0], eg, ev, ed, gains[1], gains[2], gains[3], lg, lv, ld, gains[4])


def solution(mesh):
    assert dict(mesh.shape) == {"rep": 2, "fs": 16, "tp": 4}
    rows = P(("rep", "fs", "tp"), None)
    up, down = P("fs", "tp"), P("tp", "fs")
    placed = (rows, rows, P(), up, up, down, P(), P(), P(), up, up, down, P())
    return jax.shard_map(on_device, mesh=mesh, in_specs=placed, out_specs=rows, check_vma=False)
```

```python
import functools

import jax
import jax.numpy as jnp
from jax import lax
from jax.experimental import pallas as pl
from jax.experimental.pallas import tpu as pltpu
from jax.sharding import PartitionSpec as P

epsilon = 1e-06
TILE = 256
Y, X, T = 4, 4, 4
MATRICES = 6

(
    OY1, OY2, OY3, OX1, OX2, F1, F2, X1, X3, QQ, E1, E2, OM, A2, A3, B2, C2, D1, D2, D3, D4, G1Z, G1ZM, G2Z,
    G2ZM, G3Z, G3ZM, S2, SS, ADD, OWN, FIN, GATE0, VALUE0, DOWN0, GATE1, VALUE1, DOWN1,
) = range(38)

ORDER = (
    (G1Z, 0, 0), (G1ZM, 0, 0), (OY1, 0), (OM, 0), (OY2, 0), (OX1, 0), (OX2, 0), (G2Z, 0, 0), (G2ZM, 0, 0),
    (OY3, 0), (OX1, 1), (OX2, 1), (G1Z, 0, 1), (G1ZM, 0, 1), (OY1, 1), (OM, 1), (OX1, 2), (A2, 0), (B2, 0),
    (G3Z, 0, 0), (G3ZM, 0, 0), (OY2, 1), (X1, 0), (F1, 0), (OX2, 2), (A3, 0), (B2, 1), (G2Z, 0, 1),
    (G2ZM, 0, 1), (F2, 0), (X3, 0), (G3Z, 0, 1), (G3ZM, 0, 1), (OY3, 1), (A2, 1), (D1, 0), (X1, 1), (B2, 2),
    (F1, 1), (E1, 0), (C2, 0), (F2, 1), (E2, 0), (D3, 0), (QQ, 0), (OX1, 3), (A3, 1), (D1, 1), (QQ, 1), (X3, 1),
    (OY1, 2), (OM, 2), (C2, 1), (D4, 0), (OY2, 2), (E1, 1), (D2, 0), (OY3, 2), (GATE0, 0, 1), (D2, 1), (E2, 1),
    (GATE0, 1, 3), (OX2, 3), (GATE0, 3, 4), (D3, 1), (GATE0, 4, 5), (F1, 2), (OX1, 4), (A2, 2), (F2, 2),
    (X1, 2), (D4, 1), (QQ, 2), (OX2, 4), (A3, 2), (VALUE0, 0, 1), (B2, 3), (VALUE0, 1, 2), (X3, 2), (OY1, 3),
    (OM, 3), (VALUE0, 2, 4), (OY2, 3), (VALUE0, 4, 5), (C2, 2), (D1, 2), (DOWN0, 0), (S2, 0, 0, 0),
    (SS, 0, 0, 0), (S2, 0, 0, 1), (SS, 0, 0, 1), (E1, 2), (OY3, 3), (DOWN0, 1), (D2, 2), (B2, 4), (S2, 0, 1, 0),
    (SS, 0, 1, 0), (E2, 2), (SS, 0, 1, 1), (S2, 0, 1, 1), (ADD, 0, 0, 0), (F1, 3), (OX1, 5), (A2, 3), (D3, 2),
    (ADD, 0, 0, 1), (F2, 3), (X1, 3), (ADD, 0, 1, 0), (DOWN0, 2), (S2, 0, 2, 0), (SS, 0, 2, 0), (SS, 0, 2, 1),
    (QQ, 3), (OX2, 5), (A3, 3), (ADD, 0, 1, 1), (D4, 2), (S2, 0, 2, 1), (OY1, 4), (OM, 4), (OWN, 0, 0, 0),
    (X3, 3), (OWN, 0, 1, 0), (DOWN0, 3), (S2, 0, 3, 0), (SS, 0, 3, 0), (SS, 0, 3, 1), (OY2, 4), (OWN, 0, 0, 1),
    (C2, 3), (D1, 3), (S2, 0, 3, 1), (ADD, 0, 2, 0), (OY3, 4), (E1, 3), (D2, 3), (B2, 5), (ADD, 0, 2, 1),
    (OWN, 0, 1, 1), (E2, 3), (ADD, 0, 3, 0), (F1, 4), (A2, 4), (X1, 4), (D3, 3), (ADD, 0, 3, 1), (OWN, 0, 2, 0),
    (F2, 4), (OWN, 0, 3, 0), (FIN, 0, 0), (G1Z, 1, 0), (G1ZM, 1, 0), (QQ, 4), (OWN, 0, 2, 1), (A3, 4), (X3, 4),
    (D4, 3), (OWN, 0, 3, 1), (FIN, 0, 1), (G2Z, 1, 0), (G2ZM, 1, 0), (OY1, 5), (OM, 5), (E1, 4), (D1, 4),
    (OY2, 5), (G1Z, 1, 1), (G1ZM, 1, 1), (C2, 4), (E2, 4), (OY3, 5), (D2, 4), (D3, 4), (G3Z, 1, 0),
    (G3ZM, 1, 0), (F1, 5), (A2, 5), (X1, 5), (G2Z, 1, 1), (G2ZM, 1, 1), (D4, 4), (F2, 5), (G3Z, 1, 1),
    (G3ZM, 1, 1), (QQ, 5), (A3, 5), (X3, 5), (D1, 5), (GATE1, 0, 0, 4), (E1, 5), (GATE1, 0, 4, 5),
    (VALUE1, 0, 0, 3), (C2, 5), (E2, 5), (VALUE1, 0, 3, 5), (DOWN1, 0, 0), (S2, 1, 0, 0), (SS, 1, 0, 0),
    (DOWN1, 1, 0), (D2, 5), (D3, 5), (S2, 1, 1, 0), (SS, 1, 1, 0), (GATE1, 1, 0, 4), (DOWN1, 2, 0),
    (S2, 1, 2, 0), (SS, 1, 2, 0), (GATE1, 1, 4, 5), (ADD, 1, 0, 0), (VALUE1, 1, 0, 1), (D4, 5),
    (VALUE1, 1, 1, 3), (ADD, 1, 1, 0), (VALUE1, 1, 3, 5), (DOWN1, 3, 0), (ADD, 1, 2, 0), (S2, 1, 3, 0),
    (SS, 1, 3, 0), (DOWN1, 0, 1), (SS, 1, 0, 1), (DOWN1, 1, 1), (S2, 1, 0, 1), (S2, 1, 1, 1), (DOWN1, 2, 1),
    (OWN, 1, 0, 0), (DOWN1, 3, 1), (S2, 1, 2, 1), (S2, 1, 3, 1), (OWN, 1, 1, 0), (OWN, 1, 2, 0), (ADD, 1, 3, 0),
    (SS, 1, 1, 1), (SS, 1, 3, 1), (SS, 1, 2, 1), (ADD, 1, 0, 1), (ADD, 1, 1, 1), (ADD, 1, 2, 1), (ADD, 1, 3, 1),
    (OWN, 1, 3, 0), (FIN, 1, 0), (OWN, 1, 0, 1), (OWN, 1, 1, 1), (OWN, 1, 2, 1), (OWN, 1, 3, 1), (FIN, 1, 1),
)

SETS = (((0, 0), (3, 0)), ((1, 0), (0, 1)), ((2, 0), (3, 1)), ((1, 1), (2, 1)))
SET_OF = {chip: s for s, chips in enumerate(SETS) for chip in chips}
STEPS = {
    OY1: ((), (("y+", (0, 0), 0, 1), ("y-", (0, 0), 2, 1)), "W1"),
    OY2: ((), (("y+", (0, 0), 1, 1), ("y-", (0, 0), 3, 1)), "W2"),
    OY3: ((), (("y+", (0, 0), 2, 2), ("y-", (0, 0), 0, 2)), "W3"),
    OX1: ((), (("x+", (0, 0), 0, 1), ("x-", (0, 0), 2, 1)), "X1"),
    OX2: ((), (("x+", (0, 0), 1, 1), ("x-", (0, 0), 3, 1)), "X2"),
    F1: (("W1",), (("y+", (3, 0), 0, 1), ("y-", (1, 0), 2, 1)), "F1"),
    F2: (("W2",), (("y+", (3, 0), 1, 1), ("y-", (1, 0), 3, 1)), "F2"),
    X1: (("W2",), (("x+", (3, 0), 1, 1), ("x-", (1, 0), 3, 1)), "D1"),
    X3: (("W3",), (("x-", (3, 0), 2, 2), ("x+", (1, 0), 0, 2)), "D3"),
    QQ: (("X1",), (("y+", (0, 1), 0, 1), ("y-", (0, 1), 2, 1)), "D2"),
    E1: (("F1",), (("x+", (2, 0), 0, 1), ("x-", (2, 0), 2, 1)), "E1"),
    E2: (("F2",), (("x+", (2, 0), 1, 1), ("x-", (2, 0), 3, 1)), "E2"),
    OM: ((), (("mate", (0, 0), 0, 4),), None),
    A2: (("W1", "W2"), (("mate", (3, 0), 0, 2), ("mate", (1, 0), 2, 2)), None),
    A3: (("W3",), (("mate", (3, 0), 2, 2), ("mate", (1, 0), 0, 2)), None),
    B2: (("X1", "X2"), (("mate", (0, 1), 0, 4),), None),
    C2: (("F1", "F2"), (("mate", (2, 0), 0, 4),), None),
    D1: (("D1",), (("mate", (3, 1), 1, 1), ("mate", (1, 1), 3, 1)), None),
    D2: (("D2",), (("mate", (3, 1), 0, 1), ("mate", (1, 1), 2, 1)), None),
    D3: (("D3",), (("mate", (3, 1), 2, 2), ("mate", (1, 1), 0, 2)), None),
    D4: (("E1", "E2"), (("mate", (2, 1), 0, 4),), None),
}
ARRIVALS = {arrival: sum(c[3] for c in moves) for _, moves, arrival in STEPS.values() if arrival}
SENT = sum(c[3] for _, moves, _ in STEPS.values() for c in moves)


def rms_scale(values, gain):
    scale = lax.rsqrt(jnp.mean(values * values, axis=-1, keepdims=True) + epsilon)
    return values * scale * gain


def kernel(
    tokens, mixer, early_norm, w0, w1, w2, early_post, mixer_gain, later_norm, w3, w4, w5, later_post,
    out,
    g0, g1, g2, g3, g4, g5, rows0, rows1, gate_sum, hidden, part, base, branch, mixed, from_far, from_short, from_long,
    w_send, w_recv, local_sem, z_send, z_recv,
):
    source = (w0, w1, w2, w3, w4, w5)
    full = (g0, g1, g2, g3, g4, g5)
    all_rows = (rows0, rows1)
    r, f, t = lax.axis_index("rep"), lax.axis_index("fs"), lax.axis_index("tp")
    c = f % 2
    xl = f // 2 % 2
    y = f // 4
    x = r * 2 + xl
    n, D = tokens.shape
    H = n // 2
    M = T * H
    U = H // 2

    def chip(dx, dy):
        xx = (x + dx) % X
        return {"rep": xx // 2, "fs": ((y + dy) % Y * 2 + xx % 2) * 2 + c}

    where = {
        "y+": chip(0, 1), "y-": chip(0, Y - 1), "x+": chip(1, 0), "x-": chip(X - 1, 0),
        "mate": {"fs": f + 1 - 2 * c}, "z+": {"tp": (t + 1) % T}, "z-": {"tp": (t + T - 1) % T},
    }

    def owner(chip, core):
        dy, other = chip
        return ((y + dy) % Y * 2 + (xl + other) % 2) * 2 + core

    def piece(m, shard, first, quarters):
        quarter = source[m].shape[0] // 4
        if m % 3 == 2:
            return full[m].at[shard, pl.ds(first * quarter, quarters * quarter)]
        start = pl.multiple_of(shard * 4 * quarter + first * quarter, quarter)
        return full[m].at[pl.ds(start, quarters * quarter)]

    def some(m, quarters):
        if m % 3 == 2:
            if quarters % 4 == 0:
                return full[m].at[pl.ds(0, quarters // 4)]
            return full[m].at[0, pl.ds(0, quarters * (source[m].shape[0] // 4))]
        return full[m].at[pl.ds(0, quarters * (source[m].shape[0] // 4))]

    barrier = pltpu.get_barrier_semaphore()
    for who in where.values():
        pl.semaphore_signal(barrier, inc=1, device_id=who, device_id_type=pl.DeviceIdType.MESH)
    local = []
    for m in range(MATRICES):
        local.append(pltpu.make_async_copy(source[m], piece(m, f, 0, 4), local_sem.at[m]))
        local[m].start()

    def own_rows(layer, half):
        return all_rows[layer].at[pl.ds(pl.multiple_of(half * M + t * H, H), H)]

    for half in range(2):
        at = pl.ds(half * H, H)
        own_rows(0, half)[...] = rms_scale(tokens[at].astype(jnp.float32), early_norm[...]).astype(jnp.bfloat16)
    base[...] = tokens[...].astype(jnp.float32) + rms_scale(mixer[...].astype(jnp.float32), mixer_gain[...])
    for m in range(MATRICES):
        local[m].wait()
    pl.semaphore_wait(barrier, len(where))

    slots = {"w": {}, "z": {}}
    arrived = set()

    def slot(kind, key):
        return slots[kind].setdefault(key, len(slots[kind]))

    def send(kind, src, dst, out_slot, key, way):
        sems = (w_send, w_recv) if kind == "w" else (z_send, z_recv)
        pltpu.make_async_remote_copy(
            src_ref=src, dst_ref=dst, send_sem=sems[0].at[out_slot], recv_sem=sems[1].at[slot(kind, key)],
            device_id=where[way], device_id_type=pl.DeviceIdType.MESH,
        ).start()

    def need(kind, key, same_bytes):
        if key not in arrived:
            arrived.add(key)
            sem = (w_recv if kind == "w" else z_recv).at[slot(kind, key)]
            pltpu.make_async_copy(same_bytes, same_bytes, sem).wait()

    def weights(name, m):
        waits, moves, arrival = STEPS[name]
        for key in waits:
            need("w", (key, m), some(m, ARRIVALS[key]))
        for way, chip, first, quarters in moves:
            ref = piece(m, owner(chip, c), first, quarters)
            key = arrival or ("mate", SET_OF[chip] if m % 3 == 2 else None)
            send("w", ref, ref, m, (key, m), way)

    def ready(m, s=None):
        if s is None:
            need("w", (("mate", None), m), some(m, 32))
        else:
            need("w", (("mate", s), m), some(m, 8))

    def row_piece(layer, half, block, u):
        start = pl.multiple_of(half * M + block % T * H + u * U, U)
        return all_rows[layer].at[pl.ds(start, U)]

    def gather(step, way, layer, half):
        u = (0 if way == "z+" else 1) if step != 2 else (1 if way == "z+" else 0)
        block = t
        if step == 3:
            gathered(1, layer, half)
            block = t + T - 1 if way == "z+" else t + 1
        ref = row_piece(layer, half, block, u)
        send("z", ref, ref, layer, ("rows", step, layer, half), way)

    def gathered(step, layer, half):
        need("z", ("rows", step, layer, half), all_rows[layer].at[pl.ds(0, 2 * U)])

    def all_gathered(layer, half):
        for step in (1, 2, 3):
            gathered(step, layer, half)

    def span(rows):
        return pl.ds(0, 2 * M) if rows is None else pl.ds(rows * M, M)

    def gate(layer, rows, first, last):
        weight = full[3 * layer]
        ready(3 * layer)
        for half in range(2) if rows is None else (rows,):
            all_gathered(layer, half)

        @pl.loop(first, last)
        def _(j):
            at = pl.ds(pl.multiple_of(j * TILE, TILE), TILE)
            gate_sum[span(rows), at] = jnp.dot(
                all_rows[layer][span(rows)], weight[:, at], preferred_element_type=jnp.float32
            )

    def value(layer, rows, first, last):
        weight = full[3 * layer + 1]
        ready(3 * layer + 1)

        @pl.loop(first, last)
        def _(j):
            at = pl.ds(pl.multiple_of(j * TILE, TILE), TILE)
            b = jnp.dot(all_rows[layer][span(rows)], weight[:, at], preferred_element_type=jnp.float32)
            a = gate_sum[span(rows), at]
            hidden[span(rows), at] = (a / (1.0 + jnp.exp(-a)) * b).astype(jnp.bfloat16)

    def down(layer, s, rows):
        weight = full[3 * layer + 2]
        ready(3 * layer + 2, s)
        for k, chip in enumerate(SETS[s]):
            both = jnp.concatenate([weight[owner(chip, 0)], weight[owner(chip, 1)]], axis=1)
            sums = jnp.dot(hidden[span(rows)], both, preferred_element_type=jnp.float32)
            part[layer, s, span(rows), pl.ds(k * TILE, TILE)] = sums.astype(jnp.bfloat16)

    def block(layer, s, half, b):
        return part.at[layer, s, pl.ds(pl.multiple_of(half * M + b % T * H, H), H)]

    def ways(s):
        right, left = ("z+", t + 1), ("z-", t + T - 1)
        return right + left if s % 2 == 0 else left + right

    def sum_far(layer, s, half):
        key = ("far", layer, s, half)
        send("z", block(layer, s, half, t + 2), from_far.at[layer, s, half], 2 + layer, key, ways(s)[0])

    def sum_short(layer, s, half):
        _, _, way, near = ways(s)
        key = ("own", layer, s, half)
        send("z", block(layer, s, half, near), from_short.at[layer, s, half], 2 + layer, key, way)

    def sum_long(layer, s, half):
        need("z", ("far", layer, s, half), from_far.at[layer, s, half])
        way, near, _, _ = ways(s)
        mine = block(layer, s, half, near)
        came = from_far[layer, s, half].astype(jnp.float32)
        mine[...] = (mine[...].astype(jnp.float32) + came).astype(jnp.bfloat16)
        send("z", mine, from_long.at[layer, s, half], 2 + layer, ("own", layer, s, half), way)

    def sum_own(layer, s, half):
        need("z", ("own", layer, s, half), part.at[layer, s, pl.ds(0, 2 * H)])
        total = (
            block(layer, s, half, t)[...].astype(jnp.float32)
            + from_short[layer, s, half].astype(jnp.float32)
            + from_long[layer, s, half].astype(jnp.float32)
        )
        for k, chip in enumerate(SETS[s]):
            at = pl.ds(pl.multiple_of(owner(chip, 0) * (TILE // 2), TILE), TILE)
            branch[pl.ds(half * H, H), at] = total[:, k * TILE : (k + 1) * TILE]

    def finish(layer, half):
        at = pl.ds(half * H, H)
        if layer == 0:
            keep = (base[at] + 0.5 * rms_scale(branch[at], early_post[...])).astype(jnp.bfloat16)
            mixed[at] = keep
            own_rows(1, half)[...] = rms_scale(keep.astype(jnp.float32), later_norm[...]).astype(jnp.bfloat16)
        else:
            out[at] = (
                mixed[at].astype(jnp.float32) + 0.5 * rms_scale(branch[at], later_post[...])
            ).astype(jnp.bfloat16)

    actions = {
        GATE0: lambda a, b: gate(0, None, a, b), VALUE0: lambda a, b: value(0, None, a, b),
        GATE1: lambda h, a, b: gate(1, h, a, b), VALUE1: lambda h, a, b: value(1, h, a, b),
        DOWN0: lambda s: down(0, s, None), DOWN1: lambda s, h: down(1, s, h),
        S2: sum_far, SS: sum_short, ADD: sum_long, OWN: sum_own, FIN: finish,
        G1Z: functools.partial(gather, 1, "z+"), G1ZM: functools.partial(gather, 1, "z-"),
        G2Z: functools.partial(gather, 2, "z+"), G2ZM: functools.partial(gather, 2, "z-"),
        G3Z: functools.partial(gather, 3, "z+"), G3ZM: functools.partial(gather, 3, "z-"),
    }
    for kind in STEPS:
        actions[kind] = functools.partial(weights, kind)
    for kind, *numbers in ORDER:
        actions[kind](*numbers)

    for m in range(MATRICES):
        pltpu.make_async_copy(some(m, SENT), some(m, SENT), w_send.at[m]).wait()
    for layer in range(2):
        sent = all_rows[layer].at[pl.ds(0, 12 * U)]
        pltpu.make_async_copy(sent, sent, z_send.at[layer]).wait()
        sent = part.at[layer, pl.ds(0, 3)]
        pltpu.make_async_copy(sent, sent, z_send.at[2 + layer]).wait()


def on_device(*args):
    (tokens, mixer, early_norm, eg, ev, ed, early_post, mixer_gain, later_norm, lg, lv, ld, later_post) = args
    n, D = tokens.shape
    depth, wide = eg.shape
    F = D // depth
    H = n // 2
    bf16, f32 = jnp.bfloat16, jnp.float32
    gains = [x.reshape(1, D) for x in (early_norm, early_post, mixer_gain, later_norm, later_post)]
    vmem = pl.BlockSpec(memory_space=pltpu.VMEM)
    hbm = pl.BlockSpec(memory_space=pl.ANY)
    gathered = [pltpu.VMEM((F * depth, wide), bf16)] * 2 + [pltpu.VMEM((F,) + ed.shape, bf16)]
    landing = pltpu.VMEM((2, len(SETS), 2, H, 2 * TILE), bf16)
    w_count = MATRICES * len(ARRIVALS) + 4 + 2 * len(SETS)
    z_count = 2 * 2 * (3 + 2 * len(SETS))
    return pl.pallas_call(
        kernel,
        out_shape=jax.ShapeDtypeStruct((n, D), bf16),
        in_specs=[vmem] * 3 + [hbm] * 3 + [vmem] * 3 + [hbm] * 3 + [vmem],
        out_specs=vmem,
        scratch_shapes=gathered * 2
        + [
            pltpu.VMEM((T * n, D), bf16),
            pltpu.VMEM((T * n, D), bf16),
            pltpu.VMEM((T * n, wide), f32),
            pltpu.VMEM((T * n, wide), bf16),
            pltpu.VMEM((2, len(SETS), T * n, 2 * TILE), bf16),
            pltpu.VMEM((n, D), f32),
            pltpu.VMEM((n, D), f32),
            pltpu.VMEM((n, D), bf16),
            landing,
            landing,
            landing,
            pltpu.SemaphoreType.DMA((MATRICES,)),
            pltpu.SemaphoreType.DMA((w_count,)),
            pltpu.SemaphoreType.DMA((MATRICES,)),
            pltpu.SemaphoreType.DMA((4,)),
            pltpu.SemaphoreType.DMA((z_count,)),
        ],
        compiler_params=pltpu.CompilerParams(
            collective_id=0, has_side_effects=True, vmem_limit_bytes=66_000_000
        ),
    )(tokens, mixer, gains[0], eg, ev, ed, gains[1], gains[2], gains[3], lg, lv, ld, gains[4])


def solution(mesh):
    assert dict(mesh.shape) == {"rep": 2, "fs": 16, "tp": 4}
    rows = P(("rep", "fs", "tp"), None)
    up, down = P("fs", "tp"), P("tp", "fs")
    placed = (rows, rows, P(), up, up, down, P(), P(), P(), up, up, down, P())
    return jax.shard_map(on_device, mesh=mesh, in_specs=placed, out_specs=rows, check_vma=False)
```

```python
import functools

import jax
import jax.numpy as jnp
from jax import lax
from jax.experimental import pallas as pl
from jax.experimental.pallas import tpu as pltpu
from jax.sharding import PartitionSpec as P

epsilon = 1e-06
TILE = 256
Y, X, T = 4, 4, 4
MATRICES = 6

(
    OY1, OY2, OY3, OX1, OX2, F1, F2, X1, X3, QQ, E1, E2, OM, A2, A3, B2, C2, D1, D2, D3, D4, G1Z, G1ZM, G2Z,
    G2ZM, G3Z, G3ZM, S2, SS, ADD, OWN, FIN, GATE0, VALUE0, DOWN0, GATE1, VALUE1, DOWN1, BASE, EARLY0,
    EARLY1,
) = range(41)

ORDER = (
    (G1Z, 0, 0), (OY1, 0), (OM, 0), (G1ZM, 0, 1), (OX1, 0), (OY2, 0), (OX2, 0), (BASE,), (G1Z, 0, 1),
    (G2ZM, 0, 1), (OY3, 0), (OX1, 1), (G2Z, 0, 1), (G1ZM, 0, 0), (OX2, 1), (A2, 0), (B2, 0), (F2, 0), (OX1, 2),
    (G2Z, 0, 0), (G2ZM, 0, 0), (F1, 0), (X1, 0), (A3, 0), (B2, 1), (QQ, 0), (X3, 0), (G3Z, 0, 1), (G3ZM, 0, 1),
    (OY1, 1), (OM, 1), (G3Z, 0, 0), (G3ZM, 0, 0), (C2, 0), (D1, 0), (OY2, 1), (E2, 0), (D2, 0), (OY3, 1),
    (E1, 0), (D3, 0), (OX2, 2), (A2, 1), (F1, 1), (X1, 1), (D4, 0), (F2, 1), (OX1, 3), (A3, 1), (B2, 2),
    (QQ, 1), (GATE0, 0, 1), (X3, 1), (GATE0, 1, 3), (D1, 1), (OY1, 2), (OM, 2), (GATE0, 3, 5), (C2, 1),
    (OY2, 2), (E2, 1), (D2, 1), (EARLY0, 0, 1), (OY3, 2), (E1, 1), (EARLY0, 1, 4), (D3, 1), (OX2, 3),
    (EARLY0, 4, 5), (A2, 2), (F2, 2), (X1, 2), (D4, 1), (F1, 2), (OX1, 4), (A3, 2), (B2, 3), (OY1, 3), (OM, 3),
    (VALUE0, 0, 1), (X3, 2), (VALUE0, 1, 4), (D1, 2), (OY2, 3), (VALUE0, 4, 5), (DOWN0, 0), (SS, 0, 0, 1),
    (SS, 0, 0, 0), (S2, 0, 0, 1), (S2, 0, 0, 0), (DOWN0, 1), (C2, 2), (SS, 0, 1, 1), (S2, 0, 1, 0), (E2, 2),
    (QQ, 2), (S2, 0, 1, 1), (SS, 0, 1, 0), (F1, 3), (E1, 2), (ADD, 0, 0, 1), (A2, 3), (D3, 2), (OY3, 3),
    (X1, 3), (ADD, 0, 0, 0), (D2, 2), (OX2, 4), (ADD, 0, 1, 0), (DOWN0, 2), (D4, 2), (ADD, 0, 1, 1),
    (SS, 0, 2, 0), (S2, 0, 2, 0), (S2, 0, 2, 1), (E1, 3), (F2, 3), (SS, 0, 2, 1), (OWN, 0, 0, 1), (D1, 3),
    (QQ, 3), (OX1, 5), (OWN, 0, 1, 0), (DOWN0, 3), (SS, 0, 3, 1), (S2, 0, 3, 0), (OWN, 0, 0, 0), (SS, 0, 3, 0),
    (A3, 3), (B2, 4), (QQ, 4), (X3, 3), (OWN, 0, 1, 1), (S2, 0, 3, 1), (ADD, 0, 2, 0), (C2, 3), (OY1, 4),
    (OM, 4), (ADD, 0, 2, 1), (D2, 3), (OY2, 4), (E2, 3), (ADD, 0, 3, 0), (D2, 4), (OY3, 4), (OX2, 5),
    (ADD, 0, 3, 1), (OWN, 0, 2, 0), (D3, 3), (OWN, 0, 3, 0), (FIN, 0, 0), (G1ZM, 1, 0), (G1Z, 1, 0),
    (OWN, 0, 2, 1), (A2, 4), (X1, 4), (D4, 3), (G2ZM, 1, 0), (G2Z, 1, 0), (F1, 4), (OWN, 0, 3, 1), (FIN, 0, 1),
    (B2, 5), (F2, 4), (A3, 4), (X3, 4), (D1, 4), (OY1, 5), (OM, 5), (G3ZM, 1, 0), (G3Z, 1, 0), (OY2, 5),
    (E1, 4), (G1ZM, 1, 1), (G1Z, 1, 1), (C2, 4), (OY3, 5), (E2, 4), (G2ZM, 1, 1), (G2Z, 1, 1), (D3, 4),
    (GATE1, 0, 0, 3), (A2, 5), (F1, 5), (X1, 5), (GATE1, 0, 3, 5), (EARLY1, 0, 0, 3), (D4, 4), (G3Z, 1, 1),
    (G3ZM, 1, 1), (F2, 5), (EARLY1, 0, 3, 5), (A3, 5), (X3, 5), (QQ, 5), (VALUE1, 0, 0, 1), (D1, 5),
    (VALUE1, 0, 1, 5), (DOWN1, 0, 0), (SS, 1, 0, 0), (S2, 1, 0, 0), (E1, 5), (DOWN1, 1, 0), (SS, 1, 1, 0),
    (S2, 1, 1, 0), (C2, 5), (E2, 5), (GATE1, 1, 0, 4), (D2, 5), (D3, 5), (ADD, 1, 0, 0), (GATE1, 1, 4, 5),
    (EARLY1, 1, 0, 3), (ADD, 1, 1, 0), (EARLY1, 1, 3, 5), (VALUE1, 1, 0, 2), (DOWN1, 2, 0), (SS, 1, 2, 0),
    (S2, 1, 2, 0), (VALUE1, 1, 2, 4), (D4, 5), (OWN, 1, 0, 0), (VALUE1, 1, 4, 5), (DOWN1, 0, 1), (S2, 1, 0, 1),
    (SS, 1, 0, 1), (DOWN1, 1, 1), (SS, 1, 1, 1), (S2, 1, 1, 1), (DOWN1, 2, 1), (OWN, 1, 1, 0), (SS, 1, 2, 1),
    (S2, 1, 2, 1), (DOWN1, 3, 0), (DOWN1, 3, 1), (ADD, 1, 2, 0), (S2, 1, 3, 0), (ADD, 1, 0, 1), (S2, 1, 3, 1),
    (ADD, 1, 1, 1), (SS, 1, 3, 0), (ADD, 1, 2, 1), (ADD, 1, 3, 0), (OWN, 1, 2, 0), (SS, 1, 3, 1),
    (ADD, 1, 3, 1), (OWN, 1, 0, 1), (OWN, 1, 1, 1), (OWN, 1, 3, 0), (FIN, 1, 0), (OWN, 1, 2, 1), (OWN, 1, 3, 1),
    (FIN, 1, 1),
)

SETS = (((0, 0), (3, 0)), ((1, 0), (0, 1)), ((2, 0), (3, 1)), ((1, 1), (2, 1)))
LATE = ((3, 1), (1, 1), (2, 1))
EARLY = tuple(chip for chips in SETS for chip in chips if chip not in LATE)
SET_OF = {chip: s for s, chips in enumerate(SETS) for chip in chips}
STEPS = {
    OY1: ((), (("y+", (0, 0), 0, 1), ("y-", (0, 0), 2, 1)), "W1"),
    OY2: ((), (("y+", (0, 0), 1, 1), ("y-", (0, 0), 3, 1)), "W2"),
    OY3: ((), (("y+", (0, 0), 2, 2), ("y-", (0, 0), 0, 2)), "W3"),
    OX1: ((), (("x+", (0, 0), 0, 1), ("x-", (0, 0), 2, 1)), "X1"),
    OX2: ((), (("x+", (0, 0), 1, 1), ("x-", (0, 0), 3, 1)), "X2"),
    F1: (("W1",), (("y+", (3, 0), 0, 1), ("y-", (1, 0), 2, 1)), "F1"),
    F2: (("W2",), (("y+", (3, 0), 1, 1), ("y-", (1, 0), 3, 1)), "F2"),
    X1: (("W2",), (("x+", (3, 0), 1, 1), ("x-", (1, 0), 3, 1)), "D1"),
    X3: (("W3",), (("x-", (3, 0), 2, 2), ("x+", (1, 0), 0, 2)), "D3"),
    QQ: (("X1",), (("y+", (0, 1), 0, 1), ("y-", (0, 1), 2, 1)), "D2"),
    E1: (("F1",), (("x+", (2, 0), 0, 1), ("x-", (2, 0), 2, 1)), "E1"),
    E2: (("F2",), (("x+", (2, 0), 1, 1), ("x-", (2, 0), 3, 1)), "E2"),
    OM: ((), (("mate", (0, 0), 0, 4),), None),
    A2: (("W1", "W2"), (("mate", (3, 0), 0, 2), ("mate", (1, 0), 2, 2)), None),
    A3: (("W3",), (("mate", (3, 0), 2, 2), ("mate", (1, 0), 0, 2)), None),
    B2: (("X1", "X2"), (("mate", (0, 1), 0, 4),), None),
    C2: (("F1", "F2"), (("mate", (2, 0), 0, 4),), None),
    D1: (("D1",), (("mate", (3, 1), 1, 1), ("mate", (1, 1), 3, 1)), None),
    D2: (("D2",), (("mate", (3, 1), 0, 1), ("mate", (1, 1), 2, 1)), None),
    D3: (("D3",), (("mate", (3, 1), 2, 2), ("mate", (1, 1), 0, 2)), None),
    D4: (("E1", "E2"), (("mate", (2, 1), 0, 4),), None),
}
ARRIVALS = {arrival: sum(c[3] for c in moves) for _, moves, arrival in STEPS.values() if arrival}
SENT = sum(c[3] for _, moves, _ in STEPS.values() for c in moves)


def rms_scale(values, gain):
    scale = lax.rsqrt(jnp.mean(values * values, axis=-1, keepdims=True) + epsilon)
    return values * scale * gain


def kernel(
    tokens, mixer, early_norm, w0, w1, w2, early_post, mixer_gain, later_norm, w3, w4, w5, later_post,
    out,
    g0, g1, g2, g3, g4, g5, rows0, rows1, gate_sum, value_sum, hidden, part, base, branch, mixed, from_far, from_short, from_long,
    w_send, w_recv, local_sem, z_send, z_recv,
):
    source = (w0, w1, w2, w3, w4, w5)
    full = (g0, g1, g2, g3, g4, g5)
    all_rows = (rows0, rows1)
    r, f, t = lax.axis_index("rep"), lax.axis_index("fs"), lax.axis_index("tp")
    c = f % 2
    xl = f // 2 % 2
    y = f // 4
    x = r * 2 + xl
    n, D = tokens.shape
    H = n // 2
    M = T * H
    U = H // 2

    def chip(dx, dy):
        xx = (x + dx) % X
        return {"rep": xx // 2, "fs": ((y + dy) % Y * 2 + xx % 2) * 2 + c}

    where = {
        "y+": chip(0, 1), "y-": chip(0, Y - 1), "x+": chip(1, 0), "x-": chip(X - 1, 0),
        "mate": {"fs": f + 1 - 2 * c}, "z+": {"tp": (t + 1) % T}, "z-": {"tp": (t + T - 1) % T},
    }

    def owner(chip, core):
        dy, other = chip
        return ((y + dy) % Y * 2 + (xl + other) % 2) * 2 + core

    def piece(m, shard, first, quarters):
        quarter = source[m].shape[0] // 4
        if m % 3 == 2:
            return full[m].at[shard, pl.ds(first * quarter, quarters * quarter)]
        start = pl.multiple_of(shard * 4 * quarter + first * quarter, quarter)
        return full[m].at[pl.ds(start, quarters * quarter)]

    def some(m, quarters):
        if m % 3 == 2:
            if quarters % 4 == 0:
                return full[m].at[pl.ds(0, quarters // 4)]
            return full[m].at[0, pl.ds(0, quarters * (source[m].shape[0] // 4))]
        return full[m].at[pl.ds(0, quarters * (source[m].shape[0] // 4))]

    barrier = pltpu.get_barrier_semaphore()
    for who in where.values():
        pl.semaphore_signal(barrier, inc=1, device_id=who, device_id_type=pl.DeviceIdType.MESH)
    local = []
    for m in range(MATRICES):
        local.append(pltpu.make_async_copy(source[m], piece(m, f, 0, 4), local_sem.at[m]))
        local[m].start()

    def own_rows(layer, half):
        return all_rows[layer].at[pl.ds(pl.multiple_of(half * M + t * H, H), H)]

    for half in range(2):
        at = pl.ds(half * H, H)
        own_rows(0, half)[...] = rms_scale(tokens[at].astype(jnp.float32), early_norm[...]).astype(jnp.bfloat16)
    for m in range(MATRICES):
        local[m].wait()
    pl.semaphore_wait(barrier, len(where))

    slots = {"w": {}, "z": {}}
    arrived = set()

    def slot(kind, key):
        return slots[kind].setdefault(key, len(slots[kind]))

    def send(kind, src, dst, out_slot, key, way):
        sems = (w_send, w_recv) if kind == "w" else (z_send, z_recv)
        pltpu.make_async_remote_copy(
            src_ref=src, dst_ref=dst, send_sem=sems[0].at[out_slot], recv_sem=sems[1].at[slot(kind, key)],
            device_id=where[way], device_id_type=pl.DeviceIdType.MESH,
        ).start()

    def need(kind, key, same_bytes):
        if key not in arrived:
            arrived.add(key)
            sem = (w_recv if kind == "w" else z_recv).at[slot(kind, key)]
            pltpu.make_async_copy(same_bytes, same_bytes, sem).wait()

    def weights(name, m):
        waits, moves, arrival = STEPS[name]
        for key in waits:
            need("w", (key, m), some(m, ARRIVALS[key]))
        for way, chip, first, quarters in moves:
            ref = piece(m, owner(chip, c), first, quarters)
            key = arrival or ("mate", (None, chip in LATE, SET_OF[chip])[m % 3])
            send("w", ref, ref, m, (key, m), way)

    def ready(m, s, shards):
        need("w", (("mate", s), m), some(m, 4 * shards))

    def row_piece(layer, half, block, u):
        start = pl.multiple_of(half * M + block % T * H + u * U, U)
        return all_rows[layer].at[pl.ds(start, U)]

    def gather(step, way, layer, half):
        u = (0 if way == "z+" else 1) if step != 2 else (1 if way == "z+" else 0)
        block = t
        if step == 3:
            gathered(1, layer, half)
            block = t + T - 1 if way == "z+" else t + 1
        ref = row_piece(layer, half, block, u)
        send("z", ref, ref, layer, ("rows", step, layer, half), way)

    def gathered(step, layer, half):
        need("z", ("rows", step, layer, half), all_rows[layer].at[pl.ds(0, 2 * U)])

    def all_gathered(layer, half):
        for step in (1, 2, 3):
            gathered(step, layer, half)

    def span(rows):
        return pl.ds(0, 2 * M) if rows is None else pl.ds(rows * M, M)

    def gate(layer, rows, first, last):
        weight = full[3 * layer]
        ready(3 * layer, None, 8)
        for half in range(2) if rows is None else (rows,):
            all_gathered(layer, half)

        @pl.loop(first, last)
        def _(j):
            at = pl.ds(pl.multiple_of(j * TILE, TILE), TILE)
            gate_sum[span(rows), at] = jnp.dot(
                all_rows[layer][span(rows)], weight[:, at], preferred_element_type=jnp.float32
            )

    def partial_dot(layer, rows, weight, chips, at):
        spots = [pl.ds(pl.multiple_of(owner(chip, 0) * 128, 256), 256) for chip in chips]
        left = jnp.concatenate([all_rows[layer][span(rows), spot] for spot in spots], axis=1)
        right = jnp.concatenate([weight[spot, at] for spot in spots], axis=0)
        return jnp.dot(left, right, preferred_element_type=jnp.float32)

    def value_early(layer, rows, first, last):
        weight = full[3 * layer + 1]
        ready(3 * layer + 1, False, len(EARLY))
        for half in range(2) if rows is None else (rows,):
            all_gathered(layer, half)

        @pl.loop(first, last)
        def _(j):
            at = pl.ds(pl.multiple_of(j * TILE, TILE), TILE)
            value_sum[span(rows), at] = partial_dot(layer, rows, weight, EARLY, at)

    def value(layer, rows, first, last):
        weight = full[3 * layer + 1]
        ready(3 * layer + 1, True, len(LATE))

        @pl.loop(first, last)
        def _(j):
            at = pl.ds(pl.multiple_of(j * TILE, TILE), TILE)
            b = value_sum[span(rows), at] + partial_dot(layer, rows, weight, LATE, at)
            a = gate_sum[span(rows), at]
            hidden[span(rows), at] = (a / (1.0 + jnp.exp(-a)) * b).astype(jnp.bfloat16)

    def down(layer, s, rows):
        weight = full[3 * layer + 2]
        ready(3 * layer + 2, s, 2)
        for k, chip in enumerate(SETS[s]):
            both = jnp.concatenate([weight[owner(chip, 0)], weight[owner(chip, 1)]], axis=1)
            sums = jnp.dot(hidden[span(rows)], both, preferred_element_type=jnp.float32)
            part[layer, s, span(rows), pl.ds(k * TILE, TILE)] = sums.astype(jnp.bfloat16)

    def block(layer, s, half, b):
        return part.at[layer, s, pl.ds(pl.multiple_of(half * M + b % T * H, H), H)]

    def ways(s):
        right, left = ("z+", t + 1), ("z-", t + T - 1)
        return right + left if s % 2 == 0 else left + right

    def sum_far(layer, s, half):
        key = ("far", layer, s, half)
        send("z", block(layer, s, half, t + 2), from_far.at[layer, s, half], 2 + layer, key, ways(s)[0])

    def sum_short(layer, s, half):
        _, _, way, near = ways(s)
        key = ("own", layer, s, half)
        send("z", block(layer, s, half, near), from_short.at[layer, s, half], 2 + layer, key, way)

    def sum_long(layer, s, half):
        need("z", ("far", layer, s, half), from_far.at[layer, s, half])
        way, near, _, _ = ways(s)
        mine = block(layer, s, half, near)
        came = from_far[layer, s, half].astype(jnp.float32)
        mine[...] = (mine[...].astype(jnp.float32) + came).astype(jnp.bfloat16)
        send("z", mine, from_long.at[layer, s, half], 2 + layer, ("own", layer, s, half), way)

    def sum_own(layer, s, half):
        need("z", ("own", layer, s, half), part.at[layer, s, pl.ds(0, 2 * H)])
        total = (
            block(layer, s, half, t)[...].astype(jnp.float32)
            + from_short[layer, s, half].astype(jnp.float32)
            + from_long[layer, s, half].astype(jnp.float32)
        )
        for k, chip in enumerate(SETS[s]):
            at = pl.ds(pl.multiple_of(owner(chip, 0) * (TILE // 2), TILE), TILE)
            branch[pl.ds(half * H, H), at] = total[:, k * TILE : (k + 1) * TILE]

    def start_mixed():
        base[...] = tokens[...].astype(jnp.float32) + rms_scale(mixer[...].astype(jnp.float32), mixer_gain[...])

    def finish(layer, half):
        at = pl.ds(half * H, H)
        if layer == 0:
            keep = (base[at] + 0.5 * rms_scale(branch[at], early_post[...])).astype(jnp.bfloat16)
            mixed[at] = keep
            own_rows(1, half)[...] = rms_scale(keep.astype(jnp.float32), later_norm[...]).astype(jnp.bfloat16)
        else:
            out[at] = (
                mixed[at].astype(jnp.float32) + 0.5 * rms_scale(branch[at], later_post[...])
            ).astype(jnp.bfloat16)

    actions = {
        GATE0: lambda a, b: gate(0, None, a, b), VALUE0: lambda a, b: value(0, None, a, b),
        EARLY0: lambda a, b: value_early(0, None, a, b), EARLY1: lambda h, a, b: value_early(1, h, a, b),
        GATE1: lambda h, a, b: gate(1, h, a, b), VALUE1: lambda h, a, b: value(1, h, a, b),
        DOWN0: lambda s: down(0, s, None), DOWN1: lambda s, h: down(1, s, h),
        S2: sum_far, SS: sum_short, ADD: sum_long, OWN: sum_own, FIN: finish, BASE: start_mixed,
        G1Z: functools.partial(gather, 1, "z+"), G1ZM: functools.partial(gather, 1, "z-"),
        G2Z: functools.partial(gather, 2, "z+"), G2ZM: functools.partial(gather, 2, "z-"),
        G3Z: functools.partial(gather, 3, "z+"), G3ZM: functools.partial(gather, 3, "z-"),
    }
    for kind in STEPS:
        actions[kind] = functools.partial(weights, kind)
    for kind, *numbers in ORDER:
        actions[kind](*numbers)

    for m in range(MATRICES):
        pltpu.make_async_copy(some(m, SENT), some(m, SENT), w_send.at[m]).wait()
    for layer in range(2):
        sent = all_rows[layer].at[pl.ds(0, 12 * U)]
        pltpu.make_async_copy(sent, sent, z_send.at[layer]).wait()
        sent = part.at[layer, pl.ds(0, 3)]
        pltpu.make_async_copy(sent, sent, z_send.at[2 + layer]).wait()


def on_device(*args):
    (tokens, mixer, early_norm, eg, ev, ed, early_post, mixer_gain, later_norm, lg, lv, ld, later_post) = args
    n, D = tokens.shape
    depth, wide = eg.shape
    F = D // depth
    H = n // 2
    bf16, f32 = jnp.bfloat16, jnp.float32
    gains = [x.reshape(1, D) for x in (early_norm, early_post, mixer_gain, later_norm, later_post)]
    vmem = pl.BlockSpec(memory_space=pltpu.VMEM)
    hbm = pl.BlockSpec(memory_space=pl.ANY)
    gathered = [pltpu.VMEM((F * depth, wide), bf16)] * 2 + [pltpu.VMEM((F,) + ed.shape, bf16)]
    landing = pltpu.VMEM((2, len(SETS), 2, H, 2 * TILE), bf16)
    w_count = MATRICES * len(ARRIVALS) + 6 + 2 * len(SETS)
    z_count = 2 * 2 * (3 + 2 * len(SETS))
    return pl.pallas_call(
        kernel,
        out_shape=jax.ShapeDtypeStruct((n, D), bf16),
        in_specs=[vmem] * 3 + [hbm] * 3 + [vmem] * 3 + [hbm] * 3 + [vmem],
        out_specs=vmem,
        scratch_shapes=gathered * 2
        + [
            pltpu.VMEM((T * n, D), bf16),
            pltpu.VMEM((T * n, D), bf16),
            pltpu.VMEM((T * n, wide), f32),
            pltpu.VMEM((T * n, wide), f32),
            pltpu.VMEM((T * n, wide), bf16),
            pltpu.VMEM((2, len(SETS), T * n, 2 * TILE), bf16),
            pltpu.VMEM((n, D), f32),
            pltpu.VMEM((n, D), f32),
            pltpu.VMEM((n, D), bf16),
            landing,
            landing,
            landing,
            pltpu.SemaphoreType.DMA((MATRICES,)),
            pltpu.SemaphoreType.DMA((w_count,)),
            pltpu.SemaphoreType.DMA((MATRICES,)),
            pltpu.SemaphoreType.DMA((4,)),
            pltpu.SemaphoreType.DMA((z_count,)),
        ],
        compiler_params=pltpu.CompilerParams(
            collective_id=0, has_side_effects=True, vmem_limit_bytes=66_000_000
        ),
    )(tokens, mixer, gains[0], eg, ev, ed, gains[1], gains[2], gains[3], lg, lv, ld, gains[4])


def solution(mesh):
    assert dict(mesh.shape) == {"rep": 2, "fs": 16, "tp": 4}
    rows = P(("rep", "fs", "tp"), None)
    up, down = P("fs", "tp"), P("tp", "fs")
    placed = (rows, rows, P(), up, up, down, P(), P(), P(), up, up, down, P())
    return jax.shard_map(on_device, mesh=mesh, in_specs=placed, out_specs=rows, check_vma=False)
```

```python
import functools

import jax
import jax.numpy as jnp
from jax import lax
from jax.experimental import pallas as pl
from jax.experimental.pallas import tpu as pltpu
from jax.sharding import PartitionSpec as P

epsilon = 1e-06
TILE = 256
Y, X, T = 4, 4, 4
MATRICES = 6

(
    OY1, OY2, OY3, OX1, OX2, F1, F2, X1, X3, QQ, E1, E2, OM, A2, A3, B2, C2, D1, D2, D3, D4, G1Z, G1ZM, G2Z,
    G2ZM, G3Z, G3ZM, S2, SS, ADD, OWN, FIN, GATE0, VALUE0, DOWN0, GATE1, VALUE1, DOWN1, BASE, EARLY0,
    EARLY1,
) = range(41)

ORDER = (
    (G1Z, 0, 0), (OY1, 0), (OM, 0), (G1ZM, 0, 1), (OX1, 0), (OY2, 0), (OX2, 0), (BASE,), (G1Z, 0, 1),
    (G2ZM, 0, 1), (OY3, 0), (OX1, 1), (G2Z, 0, 1), (G1ZM, 0, 0), (OX2, 1), (A2, 0), (B2, 0), (F2, 0), (OX1, 2),
    (G2Z, 0, 0), (G2ZM, 0, 0), (F1, 0), (X1, 0), (A3, 0), (B2, 1), (QQ, 0), (X3, 0), (G3Z, 0, 1), (G3ZM, 0, 1),
    (OY1, 1), (OM, 1), (G3Z, 0, 0), (G3ZM, 0, 0), (C2, 0), (D1, 0), (OY2, 1), (E2, 0), (D2, 0), (OY3, 1),
    (E1, 0), (D3, 0), (OX2, 2), (A2, 1), (F1, 1), (X1, 1), (D4, 0), (F2, 1), (OX1, 3), (A3, 1), (B2, 2),
    (QQ, 1), (GATE0, 0, 1), (X3, 1), (GATE0, 1, 3), (D1, 1), (OY1, 2), (OM, 2), (GATE0, 3, 5), (C2, 1),
    (OY2, 2), (E2, 1), (D2, 1), (EARLY0, 0, 1), (OY3, 2), (E1, 1), (EARLY0, 1, 4), (D3, 1), (OX2, 3),
    (EARLY0, 4, 5), (A2, 2), (F2, 2), (X1, 2), (D4, 1), (F1, 2), (OX1, 4), (A3, 2), (B2, 3), (OY1, 3), (OM, 3),
    (VALUE0, 0, 1), (X3, 2), (VALUE0, 1, 4), (D1, 2), (OY2, 3), (VALUE0, 4, 5), (DOWN0, 0), (SS, 0, 0, 1),
    (SS, 0, 0, 0), (S2, 0, 0, 1), (S2, 0, 0, 0), (DOWN0, 1), (C2, 2), (SS, 0, 1, 1), (S2, 0, 1, 0), (E2, 2),
    (QQ, 2), (S2, 0, 1, 1), (SS, 0, 1, 0), (F1, 3), (E1, 2), (ADD, 0, 0, 1), (A2, 3), (D3, 2), (OY3, 3),
    (X1, 3), (ADD, 0, 0, 0), (D2, 2), (OX2, 4), (ADD, 0, 1, 0), (DOWN0, 2), (D4, 2), (ADD, 0, 1, 1),
    (SS, 0, 2, 0), (S2, 0, 2, 0), (S2, 0, 2, 1), (E1, 3), (F2, 3), (SS, 0, 2, 1), (OWN, 0, 0, 1), (D1, 3),
    (QQ, 3), (OX1, 5), (OWN, 0, 1, 0), (DOWN0, 3), (SS, 0, 3, 1), (S2, 0, 3, 0), (OWN, 0, 0, 0), (SS, 0, 3, 0),
    (A3, 3), (B2, 4), (QQ, 4), (X3, 3), (OWN, 0, 1, 1), (S2, 0, 3, 1), (ADD, 0, 2, 0), (C2, 3), (OY1, 4),
    (OM, 4), (ADD, 0, 2, 1), (D2, 3), (OY2, 4), (E2, 3), (ADD, 0, 3, 0), (D2, 4), (OY3, 4), (OX2, 5),
    (ADD, 0, 3, 1), (OWN, 0, 2, 0), (D3, 3), (OWN, 0, 3, 0), (FIN, 0, 0), (G1ZM, 1, 0), (G1Z, 1, 0),
    (OWN, 0, 2, 1), (A2, 4), (X1, 4), (D4, 3), (G2ZM, 1, 0), (G2Z, 1, 0), (F1, 4), (OWN, 0, 3, 1), (FIN, 0, 1),
    (B2, 5), (F2, 4), (A3, 4), (X3, 4), (D1, 4), (OY1, 5), (OM, 5), (G3ZM, 1, 0), (G3Z, 1, 0), (OY2, 5),
    (E1, 4), (G1ZM, 1, 1), (G1Z, 1, 1), (C2, 4), (OY3, 5), (E2, 4), (G2ZM, 1, 1), (G2Z, 1, 1), (D3, 4),
    (GATE1, 0, 0, 3), (A2, 5), (F1, 5), (X1, 5), (GATE1, 0, 3, 5), (EARLY1, 0, 0, 3), (D4, 4), (G3Z, 1, 1),
    (G3ZM, 1, 1), (F2, 5), (EARLY1, 0, 3, 5), (A3, 5), (X3, 5), (QQ, 5), (VALUE1, 0, 0, 1), (D1, 5),
    (VALUE1, 0, 1, 5), (DOWN1, 0, 0), (SS, 1, 0, 0), (S2, 1, 0, 0), (E1, 5), (DOWN1, 1, 0), (SS, 1, 1, 0),
    (S2, 1, 1, 0), (C2, 5), (E2, 5), (GATE1, 1, 0, 4), (D2, 5), (D3, 5), (ADD, 1, 0, 0), (GATE1, 1, 4, 5),
    (EARLY1, 1, 0, 3), (ADD, 1, 1, 0), (EARLY1, 1, 3, 5), (VALUE1, 1, 0, 2), (DOWN1, 2, 0), (SS, 1, 2, 0),
    (S2, 1, 2, 0), (VALUE1, 1, 2, 4), (D4, 5), (OWN, 1, 0, 0), (VALUE1, 1, 4, 5), (DOWN1, 0, 1), (S2, 1, 0, 1),
    (SS, 1, 0, 1), (DOWN1, 1, 1), (SS, 1, 1, 1), (S2, 1, 1, 1), (DOWN1, 2, 1), (OWN, 1, 1, 0), (SS, 1, 2, 1),
    (S2, 1, 2, 1), (DOWN1, 3, 0), (DOWN1, 3, 1), (ADD, 1, 2, 0), (S2, 1, 3, 0), (ADD, 1, 0, 1), (S2, 1, 3, 1),
    (ADD, 1, 1, 1), (SS, 1, 3, 0), (ADD, 1, 2, 1), (ADD, 1, 3, 0), (OWN, 1, 2, 0), (SS, 1, 3, 1),
    (ADD, 1, 3, 1), (OWN, 1, 0, 1), (OWN, 1, 1, 1), (OWN, 1, 3, 0), (FIN, 1, 0), (OWN, 1, 2, 1), (OWN, 1, 3, 1),
    (FIN, 1, 1),
)

SETS = (((0, 0), (3, 0)), ((1, 0), (0, 1)), ((2, 0), (3, 1)), ((1, 1), (2, 1)))
LATE = ((3, 1), (1, 1), (2, 1))
EARLY = tuple(chip for chips in SETS for chip in chips if chip not in LATE)
SET_OF = {chip: s for s, chips in enumerate(SETS) for chip in chips}
STEPS = {
    OY1: ((), (("y+", (0, 0), 0, 1), ("y-", (0, 0), 2, 1)), "W1"),
    OY2: ((), (("y+", (0, 0), 1, 1), ("y-", (0, 0), 3, 1)), "W2"),
    OY3: ((), (("y+", (0, 0), 2, 2), ("y-", (0, 0), 0, 2)), "W3"),
    OX1: ((), (("x+", (0, 0), 0, 1), ("x-", (0, 0), 2, 1)), "X1"),
    OX2: ((), (("x+", (0, 0), 1, 1), ("x-", (0, 0), 3, 1)), "X2"),
    F1: (("W1",), (("y+", (3, 0), 0, 1), ("y-", (1, 0), 2, 1)), "F1"),
    F2: (("W2",), (("y+", (3, 0), 1, 1), ("y-", (1, 0), 3, 1)), "F2"),
    X1: (("W2",), (("x+", (3, 0), 1, 1), ("x-", (1, 0), 3, 1)), "D1"),
    X3: (("W3",), (("x-", (3, 0), 2, 2), ("x+", (1, 0), 0, 2)), "D3"),
    QQ: (("X1",), (("y+", (0, 1), 0, 1), ("y-", (0, 1), 2, 1)), "D2"),
    E1: (("F1",), (("x+", (2, 0), 0, 1), ("x-", (2, 0), 2, 1)), "E1"),
    E2: (("F2",), (("x+", (2, 0), 1, 1), ("x-", (2, 0), 3, 1)), "E2"),
    OM: ((), (("mate", (0, 0), 0, 4),), None),
    A2: (("W1", "W2"), (("mate", (3, 0), 0, 2), ("mate", (1, 0), 2, 2)), None),
    A3: (("W3",), (("mate", (3, 0), 2, 2), ("mate", (1, 0), 0, 2)), None),
    B2: (("X1", "X2"), (("mate", (0, 1), 0, 4),), None),
    C2: (("F1", "F2"), (("mate", (2, 0), 0, 4),), None),
    D1: (("D1",), (("mate", (3, 1), 1, 1), ("mate", (1, 1), 3, 1)), None),
    D2: (("D2",), (("mate", (3, 1), 0, 1), ("mate", (1, 1), 2, 1)), None),
    D3: (("D3",), (("mate", (3, 1), 2, 2), ("mate", (1, 1), 0, 2)), None),
    D4: (("E1", "E2"), (("mate", (2, 1), 0, 4),), None),
}
ARRIVALS = {arrival: sum(c[3] for c in moves) for _, moves, arrival in STEPS.values() if arrival}
SENT = sum(c[3] for _, moves, _ in STEPS.values() for c in moves)


def rms_scale(values, gain):
    scale = lax.rsqrt(jnp.mean(values * values, axis=-1, keepdims=True) + epsilon)
    return values * scale * gain


def kernel(
    tokens_in, mixer_in, early_norm_in, w0, w1, w2, early_post_in, mixer_gain_in, later_norm_in, w3, w4, w5,
    later_post_in,
    out,
    tokens, mixer, early_norm, early_post, mixer_gain, later_norm, later_post,
    g0, g1, g2, g3, g4, g5, rows0, rows1, gate_sum, value_sum, hidden, part, base, branch, mixed, from_far, from_short, from_long,
    w_send, w_recv, local_sem, z_send, z_recv,
):
    source = (w0, w1, w2, w3, w4, w5)
    full = (g0, g1, g2, g3, g4, g5)
    all_rows = (rows0, rows1)
    r, f, t = lax.axis_index("rep"), lax.axis_index("fs"), lax.axis_index("tp")
    c = f % 2
    xl = f // 2 % 2
    y = f // 4
    x = r * 2 + xl
    n, D = tokens.shape
    H = n // 2
    M = T * H
    U = H // 2

    def chip(dx, dy):
        xx = (x + dx) % X
        return {"rep": xx // 2, "fs": ((y + dy) % Y * 2 + xx % 2) * 2 + c}

    where = {
        "y+": chip(0, 1), "y-": chip(0, Y - 1), "x+": chip(1, 0), "x-": chip(X - 1, 0),
        "mate": {"fs": f + 1 - 2 * c}, "z+": {"tp": (t + 1) % T}, "z-": {"tp": (t + T - 1) % T},
    }

    def owner(chip, core):
        dy, other = chip
        return ((y + dy) % Y * 2 + (xl + other) % 2) * 2 + core

    def piece(m, shard, first, quarters):
        quarter = source[m].shape[0] // 4
        if m % 3 == 2:
            return full[m].at[shard, pl.ds(first * quarter, quarters * quarter)]
        start = pl.multiple_of(shard * 4 * quarter + first * quarter, quarter)
        return full[m].at[pl.ds(start, quarters * quarter)]

    def some(m, quarters):
        if m % 3 == 2:
            if quarters % 4 == 0:
                return full[m].at[pl.ds(0, quarters // 4)]
            return full[m].at[0, pl.ds(0, quarters * (source[m].shape[0] // 4))]
        return full[m].at[pl.ds(0, quarters * (source[m].shape[0] // 4))]

    barrier = pltpu.get_barrier_semaphore()
    for who in where.values():
        pl.semaphore_signal(barrier, inc=1, device_id=who, device_id_type=pl.DeviceIdType.MESH)
    inputs = (
        (tokens_in, tokens), (early_norm_in, early_norm), (mixer_in, mixer), (mixer_gain_in, mixer_gain),
        (early_post_in, early_post), (later_norm_in, later_norm), (later_post_in, later_post),
    )
    loads = [pltpu.make_async_copy(*pair, local_sem.at[MATRICES + k]) for k, pair in enumerate(inputs)]
    for load in loads:
        load.start()
    local = []
    for m in range(MATRICES):
        local.append(pltpu.make_async_copy(source[m], piece(m, f, 0, 4), local_sem.at[m]))
        local[m].start()

    def own_rows(layer, half):
        return all_rows[layer].at[pl.ds(pl.multiple_of(half * M + t * H, H), H)]

    for load in loads[:2]:
        load.wait()
    for half in range(2):
        at = pl.ds(half * H, H)
        own_rows(0, half)[...] = rms_scale(tokens[at].astype(jnp.float32), early_norm[...]).astype(jnp.bfloat16)
    for load in loads[2:] + local:
        load.wait()
    pl.semaphore_wait(barrier, len(where))

    slots = {"w": {}, "z": {}}
    arrived = set()

    def slot(kind, key):
        return slots[kind].setdefault(key, len(slots[kind]))

    def send(kind, src, dst, out_slot, key, way):
        sems = (w_send, w_recv) if kind == "w" else (z_send, z_recv)
        pltpu.make_async_remote_copy(
            src_ref=src, dst_ref=dst, send_sem=sems[0].at[out_slot], recv_sem=sems[1].at[slot(kind, key)],
            device_id=where[way], device_id_type=pl.DeviceIdType.MESH,
        ).start()

    def need(kind, key, same_bytes):
        if key not in arrived:
            arrived.add(key)
            sem = (w_recv if kind == "w" else z_recv).at[slot(kind, key)]
            pltpu.make_async_copy(same_bytes, same_bytes, sem).wait()

    def weights(name, m):
        waits, moves, arrival = STEPS[name]
        for key in waits:
            need("w", (key, m), some(m, ARRIVALS[key]))
        for way, chip, first, quarters in moves:
            ref = piece(m, owner(chip, c), first, quarters)
            key = arrival or ("mate", (None, chip in LATE, SET_OF[chip])[m % 3])
            send("w", ref, ref, m, (key, m), way)

    def ready(m, s, shards):
        need("w", (("mate", s), m), some(m, 4 * shards))

    def row_piece(layer, half, block, u):
        start = pl.multiple_of(half * M + block % T * H + u * U, U)
        return all_rows[layer].at[pl.ds(start, U)]

    def gather(step, way, layer, half):
        u = (0 if way == "z+" else 1) if step != 2 else (1 if way == "z+" else 0)
        block = t
        if step == 3:
            gathered(1, layer, half)
            block = t + T - 1 if way == "z+" else t + 1
        ref = row_piece(layer, half, block, u)
        send("z", ref, ref, layer, ("rows", step, layer, half), way)

    def gathered(step, layer, half):
        need("z", ("rows", step, layer, half), all_rows[layer].at[pl.ds(0, 2 * U)])

    def all_gathered(layer, half):
        for step in (1, 2, 3):
            gathered(step, layer, half)

    def span(rows):
        return pl.ds(0, 2 * M) if rows is None else pl.ds(rows * M, M)

    def gate(layer, rows, first, last):
        weight = full[3 * layer]
        ready(3 * layer, None, 8)
        for half in range(2) if rows is None else (rows,):
            all_gathered(layer, half)

        @pl.loop(first, last)
        def _(j):
            at = pl.ds(pl.multiple_of(j * TILE, TILE), TILE)
            gate_sum[span(rows), at] = jnp.dot(
                all_rows[layer][span(rows)], weight[:, at], preferred_element_type=jnp.float32
            )

    def partial_dot(layer, rows, weight, chips, at):
        spots = [pl.ds(pl.multiple_of(owner(chip, 0) * 128, 256), 256) for chip in chips]
        left = jnp.concatenate([all_rows[layer][span(rows), spot] for spot in spots], axis=1)
        right = jnp.concatenate([weight[spot, at] for spot in spots], axis=0)
        return jnp.dot(left, right, preferred_element_type=jnp.float32)

    def value_early(layer, rows, first, last):
        weight = full[3 * layer + 1]
        ready(3 * layer + 1, False, len(EARLY))
        for half in range(2) if rows is None else (rows,):
            all_gathered(layer, half)

        @pl.loop(first, last)
        def _(j):
            at = pl.ds(pl.multiple_of(j * TILE, TILE), TILE)
            value_sum[span(rows), at] = partial_dot(layer, rows, weight, EARLY, at)

    def value(layer, rows, first, last):
        weight = full[3 * layer + 1]
        ready(3 * layer + 1, True, len(LATE))

        @pl.loop(first, last)
        def _(j):
            at = pl.ds(pl.multiple_of(j * TILE, TILE), TILE)
            b = value_sum[span(rows), at] + partial_dot(layer, rows, weight, LATE, at)
            a = gate_sum[span(rows), at]
            hidden[span(rows), at] = (a / (1.0 + jnp.exp(-a)) * b).astype(jnp.bfloat16)

    def down(layer, s, rows):
        weight = full[3 * layer + 2]
        ready(3 * layer + 2, s, 2)
        for k, chip in enumerate(SETS[s]):
            both = jnp.concatenate([weight[owner(chip, 0)], weight[owner(chip, 1)]], axis=1)
            sums = jnp.dot(hidden[span(rows)], both, preferred_element_type=jnp.float32)
            part[layer, s, span(rows), pl.ds(k * TILE, TILE)] = sums.astype(jnp.bfloat16)

    def block(layer, s, half, b):
        return part.at[layer, s, pl.ds(pl.multiple_of(half * M + b % T * H, H), H)]

    def ways(s):
        right, left = ("z+", t + 1), ("z-", t + T - 1)
        return right + left if s % 2 == 0 else left + right

    def sum_far(layer, s, half):
        key = ("far", layer, s, half)
        send("z", block(layer, s, half, t + 2), from_far.at[layer, s, half], 2 + layer, key, ways(s)[0])

    def sum_short(layer, s, half):
        _, _, way, near = ways(s)
        key = ("own", layer, s, half)
        send("z", block(layer, s, half, near), from_short.at[layer, s, half], 2 + layer, key, way)

    def sum_long(layer, s, half):
        need("z", ("far", layer, s, half), from_far.at[layer, s, half])
        way, near, _, _ = ways(s)
        mine = block(layer, s, half, near)
        came = from_far[layer, s, half].astype(jnp.float32)
        mine[...] = (mine[...].astype(jnp.float32) + came).astype(jnp.bfloat16)
        send("z", mine, from_long.at[layer, s, half], 2 + layer, ("own", layer, s, half), way)

    def sum_own(layer, s, half):
        need("z", ("own", layer, s, half), part.at[layer, s, pl.ds(0, 2 * H)])
        total = (
            block(layer, s, half, t)[...].astype(jnp.float32)
            + from_short[layer, s, half].astype(jnp.float32)
            + from_long[layer, s, half].astype(jnp.float32)
        )
        for k, chip in enumerate(SETS[s]):
            at = pl.ds(pl.multiple_of(owner(chip, 0) * (TILE // 2), TILE), TILE)
            branch[pl.ds(half * H, H), at] = total[:, k * TILE : (k + 1) * TILE]

    def start_mixed():
        base[...] = tokens[...].astype(jnp.float32) + rms_scale(mixer[...].astype(jnp.float32), mixer_gain[...])

    def finish(layer, half):
        at = pl.ds(half * H, H)
        if layer == 0:
            keep = (base[at] + 0.5 * rms_scale(branch[at], early_post[...])).astype(jnp.bfloat16)
            mixed[at] = keep
            own_rows(1, half)[...] = rms_scale(keep.astype(jnp.float32), later_norm[...]).astype(jnp.bfloat16)
        else:
            out[at] = (
                mixed[at].astype(jnp.float32) + 0.5 * rms_scale(branch[at], later_post[...])
            ).astype(jnp.bfloat16)

    actions = {
        GATE0: lambda a, b: gate(0, None, a, b), VALUE0: lambda a, b: value(0, None, a, b),
        EARLY0: lambda a, b: value_early(0, None, a, b), EARLY1: lambda h, a, b: value_early(1, h, a, b),
        GATE1: lambda h, a, b: gate(1, h, a, b), VALUE1: lambda h, a, b: value(1, h, a, b),
        DOWN0: lambda s: down(0, s, None), DOWN1: lambda s, h: down(1, s, h),
        S2: sum_far, SS: sum_short, ADD: sum_long, OWN: sum_own, FIN: finish, BASE: start_mixed,
        G1Z: functools.partial(gather, 1, "z+"), G1ZM: functools.partial(gather, 1, "z-"),
        G2Z: functools.partial(gather, 2, "z+"), G2ZM: functools.partial(gather, 2, "z-"),
        G3Z: functools.partial(gather, 3, "z+"), G3ZM: functools.partial(gather, 3, "z-"),
    }
    for kind in STEPS:
        actions[kind] = functools.partial(weights, kind)
    for kind, *numbers in ORDER:
        actions[kind](*numbers)

    for m in range(MATRICES):
        pltpu.make_async_copy(some(m, SENT), some(m, SENT), w_send.at[m]).wait()
    for layer in range(2):
        sent = all_rows[layer].at[pl.ds(0, 12 * U)]
        pltpu.make_async_copy(sent, sent, z_send.at[layer]).wait()
        sent = part.at[layer, pl.ds(0, 3)]
        pltpu.make_async_copy(sent, sent, z_send.at[2 + layer]).wait()


def on_device(*args):
    (tokens, mixer, early_norm, eg, ev, ed, early_post, mixer_gain, later_norm, lg, lv, ld, later_post) = args
    n, D = tokens.shape
    depth, wide = eg.shape
    F = D // depth
    H = n // 2
    bf16, f32 = jnp.bfloat16, jnp.float32
    gains = [x.reshape(1, D) for x in (early_norm, early_post, mixer_gain, later_norm, later_post)]
    vmem = pl.BlockSpec(memory_space=pltpu.VMEM)
    hbm = pl.BlockSpec(memory_space=pl.ANY)
    gathered = [pltpu.VMEM((F * depth, wide), bf16)] * 2 + [pltpu.VMEM((F,) + ed.shape, bf16)]
    landing = pltpu.VMEM((2, len(SETS), 2, H, 2 * TILE), bf16)
    w_count = MATRICES * len(ARRIVALS) + 6 + 2 * len(SETS)
    z_count = 2 * 2 * (3 + 2 * len(SETS))
    return pl.pallas_call(
        kernel,
        out_shape=pltpu.VMEM((n, D), bf16),
        in_specs=[hbm] * len(args),
        out_specs=vmem,
        scratch_shapes=[pltpu.VMEM((n, D), bf16)] * 2
        + [pltpu.VMEM((1, D), f32)] * 5
        + gathered * 2
        + [
            pltpu.VMEM((T * n, D), bf16),
            pltpu.VMEM((T * n, D), bf16),
            pltpu.VMEM((T * n, wide), f32),
            pltpu.VMEM((T * n, wide), f32),
            pltpu.VMEM((T * n, wide), bf16),
            pltpu.VMEM((2, len(SETS), T * n, 2 * TILE), bf16),
            pltpu.VMEM((n, D), f32),
            pltpu.VMEM((n, D), f32),
            pltpu.VMEM((n, D), bf16),
            landing,
            landing,
            landing,
            pltpu.SemaphoreType.DMA((MATRICES,)),
            pltpu.SemaphoreType.DMA((w_count,)),
            pltpu.SemaphoreType.DMA((MATRICES + 7,)),
            pltpu.SemaphoreType.DMA((4,)),
            pltpu.SemaphoreType.DMA((z_count,)),
        ],
        compiler_params=pltpu.CompilerParams(
            collective_id=0, has_side_effects=True, vmem_limit_bytes=66_000_000
        ),
    )(tokens, mixer, gains[0], eg, ev, ed, gains[1], gains[2], gains[3], lg, lv, ld, gains[4])


def solution(mesh):
    assert dict(mesh.shape) == {"rep": 2, "fs": 16, "tp": 4}
    rows = P(("rep", "fs", "tp"), None)
    up, down = P("fs", "tp"), P("tp", "fs")
    placed = (rows, rows, P(), up, up, down, P(), P(), P(), up, up, down, P())
    return jax.shard_map(on_device, mesh=mesh, in_specs=placed, out_specs=rows, check_vma=False)
```

```python
import functools

import jax
import jax.numpy as jnp
from jax import lax
from jax.experimental import pallas as pl
from jax.experimental.pallas import tpu as pltpu
from jax.sharding import PartitionSpec as P

epsilon = 1e-06
TILE = 256
Y, X, T = 4, 4, 4
MATRICES = 6

(
    OY1, OY2, OY3, OX1, OX2, F1, F2, X1, X3, QQ, E1, E2, OM, A2, A3, B2, C2, D1, D2, D3, D4, G1Z, G1ZM, G2Z,
    G2ZM, G3Z, G3ZM, S2, SS, ADD, OWN, FIN, GATE0, VALUE0, DOWN0, GATE1, VALUE1, DOWN1, BASE, EARLY0,
    EARLY1, NORM,
) = range(42)

ORDER = (
    (OY1, 0), (OX1, 0), (OY2, 0), (OX2, 0), (NORM, 0), (G1Z, 0, 0), (G1ZM, 0, 0), (OY3, 0), (OM, 0), (NORM, 1),
    (G1ZM, 0, 1), (G1Z, 0, 1), (G2ZM, 0, 1), (OX1, 1), (G2Z, 0, 1), (OX2, 1), (BASE,), (A2, 0), (B2, 0),
    (F2, 0), (OX1, 2), (G2Z, 0, 0), (G2ZM, 0, 0), (F1, 0), (X1, 0), (A3, 0), (B2, 1), (QQ, 0), (X3, 0),
    (G3Z, 0, 1), (G3ZM, 0, 1), (OY1, 1), (OM, 1), (G3Z, 0, 0), (G3ZM, 0, 0), (C2, 0), (D1, 0), (OY2, 1),
    (E2, 0), (D2, 0), (OY3, 1), (E1, 0), (D3, 0), (OX2, 2), (A2, 1), (F1, 1), (X1, 1), (D4, 0), (F2, 1),
    (OX1, 3), (A3, 1), (B2, 2), (QQ, 1), (GATE0, 0, 1), (X3, 1), (GATE0, 1, 3), (D1, 1), (OY1, 2), (OM, 2),
    (GATE0, 3, 5), (C2, 1), (OY2, 2), (E2, 1), (D2, 1), (EARLY0, 0, 1), (OY3, 2), (E1, 1), (EARLY0, 1, 4),
    (D3, 1), (OX2, 3), (EARLY0, 4, 5), (A2, 2), (F2, 2), (X1, 2), (D4, 1), (F1, 2), (OX1, 4), (A3, 2), (B2, 3),
    (OY1, 3), (OM, 3), (VALUE0, 0, 1), (X3, 2), (VALUE0, 1, 4), (D1, 2), (OY2, 3), (VALUE0, 4, 5), (DOWN0, 0),
    (SS, 0, 0, 1), (SS, 0, 0, 0), (S2, 0, 0, 1), (S2, 0, 0, 0), (DOWN0, 1), (C2, 2), (SS, 0, 1, 1),
    (S2, 0, 1, 0), (E2, 2), (QQ, 2), (S2, 0, 1, 1), (SS, 0, 1, 0), (F1, 3), (E1, 2), (ADD, 0, 0, 1), (A2, 3),
    (D3, 2), (OY3, 3), (X1, 3), (ADD, 0, 0, 0), (D2, 2), (OX2, 4), (ADD, 0, 1, 0), (DOWN0, 2), (D4, 2),
    (ADD, 0, 1, 1), (SS, 0, 2, 0), (S2, 0, 2, 0), (S2, 0, 2, 1), (E1, 3), (F2, 3), (SS, 0, 2, 1),
    (OWN, 0, 0, 1), (D1, 3), (QQ, 3), (OX1, 5), (OWN, 0, 1, 0), (DOWN0, 3), (SS, 0, 3, 1), (S2, 0, 3, 0),
    (OWN, 0, 0, 0), (SS, 0, 3, 0), (A3, 3), (B2, 4), (QQ, 4), (X3, 3), (OWN, 0, 1, 1), (S2, 0, 3, 1),
    (ADD, 0, 2, 0), (C2, 3), (OY1, 4), (OM, 4), (ADD, 0, 2, 1), (D2, 3), (OY2, 4), (E2, 3), (ADD, 0, 3, 0),
    (D2, 4), (OY3, 4), (OX2, 5), (ADD, 0, 3, 1), (OWN, 0, 2, 0), (D3, 3), (OWN, 0, 3, 0), (FIN, 0, 0),
    (G1ZM, 1, 0), (G1Z, 1, 0), (OWN, 0, 2, 1), (A2, 4), (X1, 4), (D4, 3), (G2ZM, 1, 0), (G2Z, 1, 0), (F1, 4),
    (OWN, 0, 3, 1), (FIN, 0, 1), (B2, 5), (F2, 4), (A3, 4), (X3, 4), (D1, 4), (OY1, 5), (OM, 5), (G3ZM, 1, 0),
    (G3Z, 1, 0), (OY2, 5), (E1, 4), (G1ZM, 1, 1), (G1Z, 1, 1), (C2, 4), (OY3, 5), (E2, 4), (G2ZM, 1, 1),
    (G2Z, 1, 1), (D3, 4), (GATE1, 0, 0, 3), (A2, 5), (F1, 5), (X1, 5), (GATE1, 0, 3, 5), (EARLY1, 0, 0, 3),
    (D4, 4), (G3Z, 1, 1), (G3ZM, 1, 1), (F2, 5), (EARLY1, 0, 3, 5), (A3, 5), (X3, 5), (QQ, 5),
    (VALUE1, 0, 0, 1), (D1, 5), (VALUE1, 0, 1, 5), (DOWN1, 0, 0), (SS, 1, 0, 0), (S2, 1, 0, 0), (E1, 5),
    (DOWN1, 1, 0), (SS, 1, 1, 0), (S2, 1, 1, 0), (C2, 5), (E2, 5), (GATE1, 1, 0, 4), (D2, 5), (D3, 5),
    (ADD, 1, 0, 0), (GATE1, 1, 4, 5), (EARLY1, 1, 0, 3), (ADD, 1, 1, 0), (EARLY1, 1, 3, 5), (VALUE1, 1, 0, 2),
    (DOWN1, 2, 0), (SS, 1, 2, 0), (S2, 1, 2, 0), (VALUE1, 1, 2, 4), (D4, 5), (OWN, 1, 0, 0), (VALUE1, 1, 4, 5),
    (DOWN1, 0, 1), (S2, 1, 0, 1), (SS, 1, 0, 1), (DOWN1, 1, 1), (SS, 1, 1, 1), (S2, 1, 1, 1), (DOWN1, 2, 1),
    (OWN, 1, 1, 0), (SS, 1, 2, 1), (S2, 1, 2, 1), (DOWN1, 3, 0), (DOWN1, 3, 1), (ADD, 1, 2, 0), (S2, 1, 3, 0),
    (ADD, 1, 0, 1), (S2, 1, 3, 1), (ADD, 1, 1, 1), (SS, 1, 3, 0), (ADD, 1, 2, 1), (ADD, 1, 3, 0),
    (OWN, 1, 2, 0), (SS, 1, 3, 1), (ADD, 1, 3, 1), (OWN, 1, 0, 1), (OWN, 1, 1, 1), (OWN, 1, 3, 0), (FIN, 1, 0),
    (OWN, 1, 2, 1), (OWN, 1, 3, 1), (FIN, 1, 1),
)

SETS = (((0, 0), (3, 0)), ((1, 0), (0, 1)), ((2, 0), (3, 1)), ((1, 1), (2, 1)))
LATE = ((3, 1), (1, 1), (2, 1))
EARLY = tuple(chip for chips in SETS for chip in chips if chip not in LATE)
SET_OF = {chip: s for s, chips in enumerate(SETS) for chip in chips}
STEPS = {
    OY1: ((), (("y+", (0, 0), 0, 1), ("y-", (0, 0), 2, 1)), "W1"),
    OY2: ((), (("y+", (0, 0), 1, 1), ("y-", (0, 0), 3, 1)), "W2"),
    OY3: ((), (("y+", (0, 0), 2, 2), ("y-", (0, 0), 0, 2)), "W3"),
    OX1: ((), (("x+", (0, 0), 0, 1), ("x-", (0, 0), 2, 1)), "X1"),
    OX2: ((), (("x+", (0, 0), 1, 1), ("x-", (0, 0), 3, 1)), "X2"),
    F1: (("W1",), (("y+", (3, 0), 0, 1), ("y-", (1, 0), 2, 1)), "F1"),
    F2: (("W2",), (("y+", (3, 0), 1, 1), ("y-", (1, 0), 3, 1)), "F2"),
    X1: (("W2",), (("x+", (3, 0), 1, 1), ("x-", (1, 0), 3, 1)), "D1"),
    X3: (("W3",), (("x-", (3, 0), 2, 2), ("x+", (1, 0), 0, 2)), "D3"),
    QQ: (("X1",), (("y+", (0, 1), 0, 1), ("y-", (0, 1), 2, 1)), "D2"),
    E1: (("F1",), (("x+", (2, 0), 0, 1), ("x-", (2, 0), 2, 1)), "E1"),
    E2: (("F2",), (("x+", (2, 0), 1, 1), ("x-", (2, 0), 3, 1)), "E2"),
    OM: ((), (("mate", (0, 0), 0, 4),), None),
    A2: (("W1", "W2"), (("mate", (3, 0), 0, 2), ("mate", (1, 0), 2, 2)), None),
    A3: (("W3",), (("mate", (3, 0), 2, 2), ("mate", (1, 0), 0, 2)), None),
    B2: (("X1", "X2"), (("mate", (0, 1), 0, 4),), None),
    C2: (("F1", "F2"), (("mate", (2, 0), 0, 4),), None),
    D1: (("D1",), (("mate", (3, 1), 1, 1), ("mate", (1, 1), 3, 1)), None),
    D2: (("D2",), (("mate", (3, 1), 0, 1), ("mate", (1, 1), 2, 1)), None),
    D3: (("D3",), (("mate", (3, 1), 2, 2), ("mate", (1, 1), 0, 2)), None),
    D4: (("E1", "E2"), (("mate", (2, 1), 0, 4),), None),
}
ARRIVALS = {arrival: sum(c[3] for c in moves) for _, moves, arrival in STEPS.values() if arrival}
SENT = sum(c[3] for _, moves, _ in STEPS.values() for c in moves)


def rms_scale(values, gain):
    scale = lax.rsqrt(jnp.mean(values * values, axis=-1, keepdims=True) + epsilon)
    return values * scale * gain


def kernel(
    tokens_in, mixer_in, early_norm_in, w0, w1, w2, early_post_in, mixer_gain_in, later_norm_in, w3, w4, w5,
    later_post_in,
    out,
    tokens, mixer, early_norm, early_post, mixer_gain, later_norm, later_post,
    g0, g1, g2, g3, g4, g5, rows0, rows1, gate_sum, value_sum, hidden, part, base, branch, mixed, from_far, from_short, from_long,
    w_send, w_recv, local_sem, z_send, z_recv,
):
    source = (w0, w1, w2, w3, w4, w5)
    full = (g0, g1, g2, g3, g4, g5)
    all_rows = (rows0, rows1)
    r, f, t = lax.axis_index("rep"), lax.axis_index("fs"), lax.axis_index("tp")
    c = f % 2
    xl = f // 2 % 2
    y = f // 4
    x = r * 2 + xl
    n, D = tokens.shape
    H = n // 2
    M = T * H
    U = H // 2

    def chip(dx, dy):
        xx = (x + dx) % X
        return {"rep": xx // 2, "fs": ((y + dy) % Y * 2 + xx % 2) * 2 + c}

    where = {
        "y+": chip(0, 1), "y-": chip(0, Y - 1), "x+": chip(1, 0), "x-": chip(X - 1, 0),
        "mate": {"fs": f + 1 - 2 * c}, "z+": {"tp": (t + 1) % T}, "z-": {"tp": (t + T - 1) % T},
    }

    def owner(chip, core):
        dy, other = chip
        return ((y + dy) % Y * 2 + (xl + other) % 2) * 2 + core

    def piece(m, shard, first, quarters):
        quarter = source[m].shape[0] // 4
        if m % 3 == 2:
            return full[m].at[shard, pl.ds(first * quarter, quarters * quarter)]
        start = pl.multiple_of(shard * 4 * quarter + first * quarter, quarter)
        return full[m].at[pl.ds(start, quarters * quarter)]

    def some(m, quarters):
        if m % 3 == 2:
            if quarters % 4 == 0:
                return full[m].at[pl.ds(0, quarters // 4)]
            return full[m].at[0, pl.ds(0, quarters * (source[m].shape[0] // 4))]
        return full[m].at[pl.ds(0, quarters * (source[m].shape[0] // 4))]

    barrier = pltpu.get_barrier_semaphore()
    for who in where.values():
        pl.semaphore_signal(barrier, inc=1, device_id=who, device_id_type=pl.DeviceIdType.MESH)
    inputs = (
        (tokens_in, tokens), (early_norm_in, early_norm), (mixer_in, mixer), (mixer_gain_in, mixer_gain),
        (early_post_in, early_post), (later_norm_in, later_norm), (later_post_in, later_post),
    )
    loads = [pltpu.make_async_copy(*pair, local_sem.at[MATRICES + k]) for k, pair in enumerate(inputs)]
    local = [
        pltpu.make_async_copy(source[m], piece(m, f, 0, 4), local_sem.at[m]) for m in range(MATRICES)
    ]
    for load in local[:1] + loads + local[1:]:
        load.start()
    loaded = set()

    def load_wait(*copies):
        for copy in copies:
            if id(copy) not in loaded:
                loaded.add(id(copy))
                copy.wait()

    def own_rows(layer, half):
        return all_rows[layer].at[pl.ds(pl.multiple_of(half * M + t * H, H), H)]

    pl.semaphore_wait(barrier, len(where))

    slots = {"w": {}, "z": {}}
    arrived = set()

    def slot(kind, key):
        return slots[kind].setdefault(key, len(slots[kind]))

    def send(kind, src, dst, out_slot, key, way):
        sems = (w_send, w_recv) if kind == "w" else (z_send, z_recv)
        pltpu.make_async_remote_copy(
            src_ref=src, dst_ref=dst, send_sem=sems[0].at[out_slot], recv_sem=sems[1].at[slot(kind, key)],
            device_id=where[way], device_id_type=pl.DeviceIdType.MESH,
        ).start()

    def need(kind, key, same_bytes):
        if key not in arrived:
            arrived.add(key)
            sem = (w_recv if kind == "w" else z_recv).at[slot(kind, key)]
            pltpu.make_async_copy(same_bytes, same_bytes, sem).wait()

    def weights(name, m):
        waits, moves, arrival = STEPS[name]
        for key in waits:
            need("w", (key, m), some(m, ARRIVALS[key]))
        for way, chip, first, quarters in moves:
            if chip == (0, 0):
                load_wait(local[m])
            ref = piece(m, owner(chip, c), first, quarters)
            key = arrival or ("mate", (None, chip in LATE, SET_OF[chip])[m % 3])
            send("w", ref, ref, m, (key, m), way)

    def ready(m, s, shards):
        need("w", (("mate", s), m), some(m, 4 * shards))

    def row_piece(layer, half, block, u):
        start = pl.multiple_of(half * M + block % T * H + u * U, U)
        return all_rows[layer].at[pl.ds(start, U)]

    def gather(step, way, layer, half):
        u = (0 if way == "z+" else 1) if step != 2 else (1 if way == "z+" else 0)
        block = t
        if step == 3:
            gathered(1, layer, half)
            block = t + T - 1 if way == "z+" else t + 1
        ref = row_piece(layer, half, block, u)
        send("z", ref, ref, layer, ("rows", step, layer, half), way)

    def gathered(step, layer, half):
        need("z", ("rows", step, layer, half), all_rows[layer].at[pl.ds(0, 2 * U)])

    def all_gathered(layer, half):
        for step in (1, 2, 3):
            gathered(step, layer, half)

    def span(rows):
        return pl.ds(0, 2 * M) if rows is None else pl.ds(rows * M, M)

    def gate(layer, rows, first, last):
        weight = full[3 * layer]
        ready(3 * layer, None, 8)
        for half in range(2) if rows is None else (rows,):
            all_gathered(layer, half)

        @pl.loop(first, last)
        def _(j):
            at = pl.ds(pl.multiple_of(j * TILE, TILE), TILE)
            gate_sum[span(rows), at] = jnp.dot(
                all_rows[layer][span(rows)], weight[:, at], preferred_element_type=jnp.float32
            )

    def partial_dot(layer, rows, weight, chips, at):
        spots = [pl.ds(pl.multiple_of(owner(chip, 0) * 128, 256), 256) for chip in chips]
        left = jnp.concatenate([all_rows[layer][span(rows), spot] for spot in spots], axis=1)
        right = jnp.concatenate([weight[spot, at] for spot in spots], axis=0)
        return jnp.dot(left, right, preferred_element_type=jnp.float32)

    def value_early(layer, rows, first, last):
        weight = full[3 * layer + 1]
        ready(3 * layer + 1, False, len(EARLY))
        for half in range(2) if rows is None else (rows,):
            all_gathered(layer, half)

        @pl.loop(first, last)
        def _(j):
            at = pl.ds(pl.multiple_of(j * TILE, TILE), TILE)
            value_sum[span(rows), at] = partial_dot(layer, rows, weight, EARLY, at)

    def value(layer, rows, first, last):
        weight = full[3 * layer + 1]
        ready(3 * layer + 1, True, len(LATE))

        @pl.loop(first, last)
        def _(j):
            at = pl.ds(pl.multiple_of(j * TILE, TILE), TILE)
            b = value_sum[span(rows), at] + partial_dot(layer, rows, weight, LATE, at)
            a = gate_sum[span(rows), at]
            hidden[span(rows), at] = (a / (1.0 + jnp.exp(-a)) * b).astype(jnp.bfloat16)

    def down(layer, s, rows):
        weight = full[3 * layer + 2]
        ready(3 * layer + 2, s, 2)
        for k, chip in enumerate(SETS[s]):
            both = jnp.concatenate([weight[owner(chip, 0)], weight[owner(chip, 1)]], axis=1)
            sums = jnp.dot(hidden[span(rows)], both, preferred_element_type=jnp.float32)
            part[layer, s, span(rows), pl.ds(k * TILE, TILE)] = sums.astype(jnp.bfloat16)

    def block(layer, s, half, b):
        return part.at[layer, s, pl.ds(pl.multiple_of(half * M + b % T * H, H), H)]

    def ways(s):
        right, left = ("z+", t + 1), ("z-", t + T - 1)
        return right + left if s % 2 == 0 else left + right

    def sum_far(layer, s, half):
        key = ("far", layer, s, half)
        send("z", block(layer, s, half, t + 2), from_far.at[layer, s, half], 2 + layer, key, ways(s)[0])

    def sum_short(layer, s, half):
        _, _, way, near = ways(s)
        key = ("own", layer, s, half)
        send("z", block(layer, s, half, near), from_short.at[layer, s, half], 2 + layer, key, way)

    def sum_long(layer, s, half):
        need("z", ("far", layer, s, half), from_far.at[layer, s, half])
        way, near, _, _ = ways(s)
        mine = block(layer, s, half, near)
        came = from_far[layer, s, half].astype(jnp.float32)
        mine[...] = (mine[...].astype(jnp.float32) + came).astype(jnp.bfloat16)
        send("z", mine, from_long.at[layer, s, half], 2 + layer, ("own", layer, s, half), way)

    def sum_own(layer, s, half):
        need("z", ("own", layer, s, half), part.at[layer, s, pl.ds(0, 2 * H)])
        total = (
            block(layer, s, half, t)[...].astype(jnp.float32)
            + from_short[layer, s, half].astype(jnp.float32)
            + from_long[layer, s, half].astype(jnp.float32)
        )
        for k, chip in enumerate(SETS[s]):
            at = pl.ds(pl.multiple_of(owner(chip, 0) * (TILE // 2), TILE), TILE)
            branch[pl.ds(half * H, H), at] = total[:, k * TILE : (k + 1) * TILE]

    def norm(half):
        load_wait(*loads[:2])
        at = pl.ds(half * H, H)
        own_rows(0, half)[...] = rms_scale(tokens[at].astype(jnp.float32), early_norm[...]).astype(jnp.bfloat16)

    def start_mixed():
        load_wait(*loads)
        base[...] = tokens[...].astype(jnp.float32) + rms_scale(mixer[...].astype(jnp.float32), mixer_gain[...])

    def finish(layer, half):
        at = pl.ds(half * H, H)
        if layer == 0:
            keep = (base[at] + 0.5 * rms_scale(branch[at], early_post[...])).astype(jnp.bfloat16)
            mixed[at] = keep
            own_rows(1, half)[...] = rms_scale(keep.astype(jnp.float32), later_norm[...]).astype(jnp.bfloat16)
        else:
            out[at] = (
                mixed[at].astype(jnp.float32) + 0.5 * rms_scale(branch[at], later_post[...])
            ).astype(jnp.bfloat16)

    actions = {
        GATE0: lambda a, b: gate(0, None, a, b), VALUE0: lambda a, b: value(0, None, a, b),
        EARLY0: lambda a, b: value_early(0, None, a, b), EARLY1: lambda h, a, b: value_early(1, h, a, b),
        GATE1: lambda h, a, b: gate(1, h, a, b), VALUE1: lambda h, a, b: value(1, h, a, b),
        DOWN0: lambda s: down(0, s, None), DOWN1: lambda s, h: down(1, s, h),
        S2: sum_far, SS: sum_short, ADD: sum_long, OWN: sum_own, FIN: finish, BASE: start_mixed, NORM: norm,
        G1Z: functools.partial(gather, 1, "z+"), G1ZM: functools.partial(gather, 1, "z-"),
        G2Z: functools.partial(gather, 2, "z+"), G2ZM: functools.partial(gather, 2, "z-"),
        G3Z: functools.partial(gather, 3, "z+"), G3ZM: functools.partial(gather, 3, "z-"),
    }
    for kind in STEPS:
        actions[kind] = functools.partial(weights, kind)
    for kind, *numbers in ORDER:
        actions[kind](*numbers)

    for m in range(MATRICES):
        pltpu.make_async_copy(some(m, SENT), some(m, SENT), w_send.at[m]).wait()
    for layer in range(2):
        sent = all_rows[layer].at[pl.ds(0, 12 * U)]
        pltpu.make_async_copy(sent, sent, z_send.at[layer]).wait()
        sent = part.at[layer, pl.ds(0, 3)]
        pltpu.make_async_copy(sent, sent, z_send.at[2 + layer]).wait()


def on_device(*args):
    (tokens, mixer, early_norm, eg, ev, ed, early_post, mixer_gain, later_norm, lg, lv, ld, later_post) = args
    n, D = tokens.shape
    depth, wide = eg.shape
    F = D // depth
    H = n // 2
    bf16, f32 = jnp.bfloat16, jnp.float32
    gains = [x.reshape(1, D) for x in (early_norm, early_post, mixer_gain, later_norm, later_post)]
    vmem = pl.BlockSpec(memory_space=pltpu.VMEM)
    hbm = pl.BlockSpec(memory_space=pl.ANY)
    gathered = [pltpu.VMEM((F * depth, wide), bf16)] * 2 + [pltpu.VMEM((F,) + ed.shape, bf16)]
    landing = pltpu.VMEM((2, len(SETS), 2, H, 2 * TILE), bf16)
    w_count = MATRICES * len(ARRIVALS) + 6 + 2 * len(SETS)
    z_count = 2 * 2 * (3 + 2 * len(SETS))
    return pl.pallas_call(
        kernel,
        out_shape=pltpu.VMEM((n, D), bf16),
        in_specs=[hbm] * len(args),
        out_specs=vmem,
        scratch_shapes=[pltpu.VMEM((n, D), bf16)] * 2
        + [pltpu.VMEM((1, D), f32)] * 5
        + gathered * 2
        + [
            pltpu.VMEM((T * n, D), bf16),
            pltpu.VMEM((T * n, D), bf16),
            pltpu.VMEM((T * n, wide), f32),
            pltpu.VMEM((T * n, wide), f32),
            pltpu.VMEM((T * n, wide), bf16),
            pltpu.VMEM((2, len(SETS), T * n, 2 * TILE), bf16),
            pltpu.VMEM((n, D), f32),
            pltpu.VMEM((n, D), f32),
            pltpu.VMEM((n, D), bf16),
            landing,
            landing,
            landing,
            pltpu.SemaphoreType.DMA((MATRICES,)),
            pltpu.SemaphoreType.DMA((w_count,)),
            pltpu.SemaphoreType.DMA((MATRICES + 7,)),
            pltpu.SemaphoreType.DMA((4,)),
            pltpu.SemaphoreType.DMA((z_count,)),
        ],
        compiler_params=pltpu.CompilerParams(
            collective_id=0, has_side_effects=True, vmem_limit_bytes=66_000_000
        ),
    )(tokens, mixer, gains[0], eg, ev, ed, gains[1], gains[2], gains[3], lg, lv, ld, gains[4])


def solution(mesh):
    assert dict(mesh.shape) == {"rep": 2, "fs": 16, "tp": 4}
    rows = P(("rep", "fs", "tp"), None)
    up, down = P("fs", "tp"), P("tp", "fs")
    placed = (rows, rows, P(), up, up, down, P(), P(), P(), up, up, down, P())
    return jax.shard_map(on_device, mesh=mesh, in_specs=placed, out_specs=rows, check_vma=False)
```

```python
import functools

import jax
import jax.numpy as jnp
from jax import lax
from jax.experimental import pallas as pl
from jax.experimental.pallas import tpu as pltpu
from jax.sharding import PartitionSpec as P

epsilon = 1e-06
TILE = 256
Y, X, T = 4, 4, 4
MATRICES = 6

(
    OY1, OY2, OY3, OX1, OX2, F1, F2, X1, X3, QQ, E1, E2, OM, A2, A3, B2, C2, D1, D2, D3, D4, G1Z, G1ZM, G2Z,
    G2ZM, G3Z, G3ZM, S2, SS, ADD, OWN, FIN, GATE0, VALUE0, DOWN0, GATE1, VALUE1, DOWN1, BASE, EARLY0,
    EARLY1, NORM,
) = range(42)

ORDER = (
    (OY1, 0), (OM, 0), (OX1, 0), (OY2, 0), (OX2, 0), (NORM, 0), (G1Z, 0, 0), (G1ZM, 0, 0), (NORM, 1),
    (G1Z, 0, 1), (G1ZM, 0, 1), (BASE,), (OY3, 0), (OX1, 1), (G2Z, 0, 1), (G2ZM, 0, 1), (OX2, 1), (A2, 0),
    (F2, 0), (B2, 0), (OX1, 2), (G2Z, 0, 0), (G2ZM, 0, 0), (F1, 0), (X1, 0), (G3Z, 0, 1), (G3ZM, 0, 1), (A3, 0),
    (QQ, 0), (B2, 1), (X3, 0), (OY1, 1), (OM, 1), (G3Z, 0, 0), (G3ZM, 0, 0), (C2, 0), (OY2, 1), (D1, 0),
    (E2, 0), (D2, 0), (OY3, 1), (E1, 0), (D3, 0), (OX2, 2), (A2, 1), (F1, 1), (X1, 1), (QQ, 1), (D4, 0),
    (OX1, 3), (GATE0, 0, 1), (A3, 1), (B2, 2), (F2, 1), (X3, 1), (GATE0, 1, 3), (D1, 1), (OY1, 2), (OM, 2),
    (GATE0, 3, 5), (D2, 1), (OY2, 2), (E1, 1), (C2, 1), (OY3, 2), (E2, 1), (EARLY0, 0, 1), (D3, 1), (OX2, 3),
    (EARLY0, 1, 4), (A2, 2), (X1, 2), (F2, 2), (EARLY0, 4, 5), (F1, 2), (D4, 1), (OX1, 4), (VALUE0, 0, 1),
    (A3, 2), (B2, 3), (X3, 2), (OY1, 3), (OM, 3), (VALUE0, 1, 4), (D1, 2), (OY2, 3), (VALUE0, 4, 5), (DOWN0, 0),
    (SS, 0, 0, 1), (SS, 0, 0, 0), (S2, 0, 0, 1), (S2, 0, 0, 0), (DOWN0, 1), (C2, 2), (E2, 2), (S2, 0, 1, 0),
    (SS, 0, 1, 1), (QQ, 2), (S2, 0, 1, 1), (SS, 0, 1, 0), (F1, 3), (E1, 2), (ADD, 0, 0, 1), (A2, 3), (OY3, 3),
    (D3, 2), (X1, 3), (ADD, 0, 0, 0), (D2, 2), (OX2, 4), (ADD, 0, 1, 0), (DOWN0, 2), (D4, 2), (ADD, 0, 1, 1),
    (SS, 0, 2, 0), (S2, 0, 2, 0), (S2, 0, 2, 1), (SS, 0, 2, 1), (F2, 3), (E1, 3), (OWN, 0, 0, 1), (QQ, 3),
    (D1, 3), (OX1, 5), (OWN, 0, 1, 0), (DOWN0, 3), (S2, 0, 3, 0), (SS, 0, 3, 1), (SS, 0, 3, 0), (OWN, 0, 0, 0),
    (S2, 0, 3, 1), (A3, 3), (OY1, 4), (OM, 4), (B2, 4), (X3, 3), (OWN, 0, 1, 1), (ADD, 0, 2, 0), (C2, 3),
    (QQ, 4), (ADD, 0, 2, 1), (D2, 3), (OY2, 4), (E2, 3), (ADD, 0, 3, 0), (OY3, 4), (OX2, 5), (ADD, 0, 3, 1),
    (OWN, 0, 2, 0), (D2, 4), (D3, 3), (OWN, 0, 2, 1), (OWN, 0, 3, 0), (FIN, 0, 0), (G1Z, 1, 0), (G1ZM, 1, 0),
    (G2ZM, 1, 0), (G2Z, 1, 0), (A2, 4), (X1, 4), (D4, 3), (F1, 4), (OWN, 0, 3, 1), (FIN, 0, 1), (F2, 4),
    (B2, 5), (A3, 4), (X3, 4), (OY1, 5), (OM, 5), (D1, 4), (G3Z, 1, 0), (G3ZM, 1, 0), (G1Z, 1, 1), (G1ZM, 1, 1),
    (OY2, 5), (E1, 4), (C2, 4), (OY3, 5), (E2, 4), (G2Z, 1, 1), (G2ZM, 1, 1), (D3, 4), (GATE1, 0, 0, 2),
    (A2, 5), (X1, 5), (F1, 5), (GATE1, 0, 2, 5), (EARLY1, 0, 0, 1), (F2, 5), (EARLY1, 0, 1, 2), (D4, 4),
    (EARLY1, 0, 2, 3), (G3ZM, 1, 1), (G3Z, 1, 1), (EARLY1, 0, 3, 5), (A3, 5), (X3, 5), (QQ, 5),
    (VALUE1, 0, 0, 1), (D1, 5), (VALUE1, 0, 1, 5), (DOWN1, 0, 0), (SS, 1, 0, 0), (S2, 1, 0, 0), (E1, 5),
    (DOWN1, 1, 0), (SS, 1, 1, 0), (S2, 1, 1, 0), (C2, 5), (E2, 5), (GATE1, 1, 0, 3), (D2, 5), (D3, 5),
    (GATE1, 1, 3, 4), (ADD, 1, 0, 0), (GATE1, 1, 4, 5), (EARLY1, 1, 0, 3), (ADD, 1, 1, 0), (EARLY1, 1, 3, 4),
    (DOWN1, 2, 0), (SS, 1, 2, 0), (S2, 1, 2, 0), (EARLY1, 1, 4, 5), (VALUE1, 1, 0, 3), (D4, 5),
    (VALUE1, 1, 3, 4), (OWN, 1, 0, 0), (VALUE1, 1, 4, 5), (DOWN1, 0, 1), (SS, 1, 0, 1), (S2, 1, 0, 1),
    (DOWN1, 1, 1), (S2, 1, 1, 1), (SS, 1, 1, 1), (DOWN1, 2, 1), (SS, 1, 2, 1), (S2, 1, 2, 1), (OWN, 1, 1, 0),
    (DOWN1, 3, 0), (DOWN1, 3, 1), (ADD, 1, 2, 0), (S2, 1, 3, 0), (SS, 1, 3, 0), (S2, 1, 3, 1), (ADD, 1, 0, 1),
    (ADD, 1, 1, 1), (SS, 1, 3, 1), (ADD, 1, 2, 1), (OWN, 1, 2, 0), (ADD, 1, 3, 0), (ADD, 1, 3, 1),
    (OWN, 1, 0, 1), (OWN, 1, 1, 1), (OWN, 1, 3, 0), (FIN, 1, 0), (OWN, 1, 2, 1), (OWN, 1, 3, 1), (FIN, 1, 1),
)

SETS = (((0, 0), (3, 0)), ((1, 0), (0, 1)), ((2, 0), (3, 1)), ((1, 1), (2, 1)))
LATE = ((3, 1), (1, 1), (2, 1))
EARLY = tuple(chip for chips in SETS for chip in chips if chip not in LATE)
SET_OF = {chip: s for s, chips in enumerate(SETS) for chip in chips}
STEPS = {
    OY1: ((), (("y+", (0, 0), 0, 1), ("y-", (0, 0), 2, 1)), "W1"),
    OY2: ((), (("y+", (0, 0), 1, 1), ("y-", (0, 0), 3, 1)), "W2"),
    OY3: ((), (("y+", (0, 0), 2, 2), ("y-", (0, 0), 0, 2)), "W3"),
    OX1: ((), (("x+", (0, 0), 0, 1), ("x-", (0, 0), 2, 1)), "X1"),
    OX2: ((), (("x+", (0, 0), 1, 1), ("x-", (0, 0), 3, 1)), "X2"),
    F1: (("W1",), (("y+", (3, 0), 0, 1), ("y-", (1, 0), 2, 1)), "F1"),
    F2: (("W2",), (("y+", (3, 0), 1, 1), ("y-", (1, 0), 3, 1)), "F2"),
    X1: (("W2",), (("x+", (3, 0), 1, 1), ("x-", (1, 0), 3, 1)), "D1"),
    X3: (("W3",), (("x-", (3, 0), 2, 2), ("x+", (1, 0), 0, 2)), "D3"),
    QQ: (("X1",), (("y+", (0, 1), 0, 1), ("y-", (0, 1), 2, 1)), "D2"),
    E1: (("F1",), (("x+", (2, 0), 0, 1), ("x-", (2, 0), 2, 1)), "E1"),
    E2: (("F2",), (("x+", (2, 0), 1, 1), ("x-", (2, 0), 3, 1)), "E2"),
    OM: ((), (("mate", (0, 0), 0, 4),), None),
    A2: (("W1", "W2"), (("mate", (3, 0), 0, 2), ("mate", (1, 0), 2, 2)), None),
    A3: (("W3",), (("mate", (3, 0), 2, 2), ("mate", (1, 0), 0, 2)), None),
    B2: (("X1", "X2"), (("mate", (0, 1), 0, 4),), None),
    C2: (("F1", "F2"), (("mate", (2, 0), 0, 4),), None),
    D1: (("D1",), (("mate", (3, 1), 1, 1), ("mate", (1, 1), 3, 1)), None),
    D2: (("D2",), (("mate", (3, 1), 0, 1), ("mate", (1, 1), 2, 1)), None),
    D3: (("D3",), (("mate", (3, 1), 2, 2), ("mate", (1, 1), 0, 2)), None),
    D4: (("E1", "E2"), (("mate", (2, 1), 0, 4),), None),
}
ARRIVALS = {arrival: sum(c[3] for c in moves) for _, moves, arrival in STEPS.values() if arrival}
SENT = sum(c[3] for _, moves, _ in STEPS.values() for c in moves)


def rms_scale(values, gain):
    scale = lax.rsqrt(jnp.mean(values * values, axis=-1, keepdims=True) + epsilon)
    return values * scale * gain


def kernel(
    tokens_in, mixer_in, early_norm_in, w0, w1, w2, early_post_in, mixer_gain_in, later_norm_in, w3, w4, w5,
    later_post_in,
    out,
    tokens, mixer, early_norm, early_post, mixer_gain, later_norm, later_post,
    g0, g1, g2, g3, g4, g5, rows0, rows1, gate_sum, value_sum, hidden, part, base, branch, mixed, from_far, from_short, from_long,
    w_send, w_recv, local_sem, z_send, z_recv,
):
    source = (w0, w1, w2, w3, w4, w5)
    full = (g0, g1, g2, g3, g4, g5)
    all_rows = (rows0, rows1)
    r, f, t = lax.axis_index("rep"), lax.axis_index("fs"), lax.axis_index("tp")
    c = f % 2
    xl = f // 2 % 2
    y = f // 4
    x = r * 2 + xl
    n, D = tokens.shape
    H = n // 2
    M = T * H
    U = H // 2

    def chip(dx, dy):
        xx = (x + dx) % X
        return {"rep": xx // 2, "fs": ((y + dy) % Y * 2 + xx % 2) * 2 + c}

    where = {
        "y+": chip(0, 1), "y-": chip(0, Y - 1), "x+": chip(1, 0), "x-": chip(X - 1, 0),
        "mate": {"fs": f + 1 - 2 * c}, "z+": {"tp": (t + 1) % T}, "z-": {"tp": (t + T - 1) % T},
    }

    def owner(chip, core):
        dy, other = chip
        return ((y + dy) % Y * 2 + (xl + other) % 2) * 2 + core

    def piece(m, shard, first, quarters):
        quarter = source[m].shape[0] // 4
        if m % 3 == 2:
            return full[m].at[shard, pl.ds(first * quarter, quarters * quarter)]
        start = pl.multiple_of(shard * 4 * quarter + first * quarter, quarter)
        return full[m].at[pl.ds(start, quarters * quarter)]

    def some(m, quarters):
        if m % 3 == 2:
            if quarters % 4 == 0:
                return full[m].at[pl.ds(0, quarters // 4)]
            return full[m].at[0, pl.ds(0, quarters * (source[m].shape[0] // 4))]
        return full[m].at[pl.ds(0, quarters * (source[m].shape[0] // 4))]

    barrier = pltpu.get_barrier_semaphore()
    for who in where.values():
        pl.semaphore_signal(barrier, inc=1, device_id=who, device_id_type=pl.DeviceIdType.MESH)
    inputs = (
        (tokens_in, tokens), (early_norm_in, early_norm), (mixer_in, mixer), (mixer_gain_in, mixer_gain),
        (early_post_in, early_post), (later_norm_in, later_norm), (later_post_in, later_post),
    )
    loads = [pltpu.make_async_copy(*pair, local_sem.at[MATRICES + k]) for k, pair in enumerate(inputs)]
    local = [
        pltpu.make_async_copy(source[m], piece(m, f, 0, 4), local_sem.at[m]) for m in range(MATRICES)
    ]
    for load in local[:1] + loads + local[1:]:
        load.start()
    loaded = set()

    def load_wait(*copies):
        for copy in copies:
            if id(copy) not in loaded:
                loaded.add(id(copy))
                copy.wait()

    def own_rows(layer, half):
        return all_rows[layer].at[pl.ds(pl.multiple_of(half * M + t * H, H), H)]

    pl.semaphore_wait(barrier, len(where))

    slots = {"w": {}, "z": {}}
    arrived = set()

    def slot(kind, key):
        return slots[kind].setdefault(key, len(slots[kind]))

    def send(kind, src, dst, out_slot, key, way):
        sems = (w_send, w_recv) if kind == "w" else (z_send, z_recv)
        pltpu.make_async_remote_copy(
            src_ref=src, dst_ref=dst, send_sem=sems[0].at[out_slot], recv_sem=sems[1].at[slot(kind, key)],
            device_id=where[way], device_id_type=pl.DeviceIdType.MESH,
        ).start()

    def need(kind, key, same_bytes):
        if key not in arrived:
            arrived.add(key)
            sem = (w_recv if kind == "w" else z_recv).at[slot(kind, key)]
            pltpu.make_async_copy(same_bytes, same_bytes, sem).wait()

    def weights(name, m):
        waits, moves, arrival = STEPS[name]
        for key in waits:
            need("w", (key, m), some(m, ARRIVALS[key]))
        for way, chip, first, quarters in moves:
            if chip == (0, 0):
                load_wait(local[m])
            ref = piece(m, owner(chip, c), first, quarters)
            key = arrival or ("mate", (None, chip in LATE, SET_OF[chip])[m % 3])
            send("w", ref, ref, m, (key, m), way)

    def ready(m, s, shards):
        need("w", (("mate", s), m), some(m, 4 * shards))

    def row_piece(layer, half, block, u):
        start = pl.multiple_of(half * M + block % T * H + u * U, U)
        return all_rows[layer].at[pl.ds(start, U)]

    def gather(step, way, layer, half):
        u = (0 if way == "z+" else 1) if step != 2 else (1 if way == "z+" else 0)
        block = t
        if step == 3:
            gathered(1, layer, half)
            block = t + T - 1 if way == "z+" else t + 1
        ref = row_piece(layer, half, block, u)
        send("z", ref, ref, layer, ("rows", step, layer, half), way)

    def gathered(step, layer, half):
        need("z", ("rows", step, layer, half), all_rows[layer].at[pl.ds(0, 2 * U)])

    def all_gathered(layer, half):
        for step in (1, 2, 3):
            gathered(step, layer, half)

    def span(rows):
        return pl.ds(0, 2 * M) if rows is None else pl.ds(rows * M, M)

    def gate(layer, rows, first, last):
        weight = full[3 * layer]
        ready(3 * layer, None, 8)
        for half in range(2) if rows is None else (rows,):
            all_gathered(layer, half)

        @pl.loop(first, last)
        def _(j):
            at = pl.ds(pl.multiple_of(j * TILE, TILE), TILE)
            gate_sum[span(rows), at] = jnp.dot(
                all_rows[layer][span(rows)], weight[:, at], preferred_element_type=jnp.float32
            )

    def partial_dot(layer, rows, weight, chips, at):
        spots = [pl.ds(pl.multiple_of(owner(chip, 0) * 128, 256), 256) for chip in chips]
        left = jnp.concatenate([all_rows[layer][span(rows), spot] for spot in spots], axis=1)
        right = jnp.concatenate([weight[spot, at] for spot in spots], axis=0)
        return jnp.dot(left, right, preferred_element_type=jnp.float32)

    def value_early(layer, rows, first, last):
        weight = full[3 * layer + 1]
        ready(3 * layer + 1, False, len(EARLY))
        for half in range(2) if rows is None else (rows,):
            all_gathered(layer, half)

        @pl.loop(first, last)
        def _(j):
            at = pl.ds(pl.multiple_of(j * TILE, TILE), TILE)
            value_sum[span(rows), at] = partial_dot(layer, rows, weight, EARLY, at)

    def value(layer, rows, first, last):
        weight = full[3 * layer + 1]
        ready(3 * layer + 1, True, len(LATE))

        @pl.loop(first, last)
        def _(j):
            at = pl.ds(pl.multiple_of(j * TILE, TILE), TILE)
            b = value_sum[span(rows), at] + partial_dot(layer, rows, weight, LATE, at)
            a = gate_sum[span(rows), at]
            hidden[span(rows), at] = (a / (1.0 + jnp.exp(-a)) * b).astype(jnp.bfloat16)

    def down(layer, s, rows):
        weight = full[3 * layer + 2]
        ready(3 * layer + 2, s, 2)
        for k, chip in enumerate(SETS[s]):
            both = jnp.concatenate([weight[owner(chip, 0)], weight[owner(chip, 1)]], axis=1)
            sums = jnp.dot(hidden[span(rows)], both, preferred_element_type=jnp.float32)
            part[layer, s, span(rows), pl.ds(k * TILE, TILE)] = sums.astype(jnp.bfloat16)

    def block(layer, s, half, b):
        return part.at[layer, s, pl.ds(pl.multiple_of(half * M + b % T * H, H), H)]

    def ways(s):
        right, left = ("z+", t + 1), ("z-", t + T - 1)
        return right + left if s % 2 == 0 else left + right

    def sum_far(layer, s, half):
        key = ("far", layer, s, half)
        send("z", block(layer, s, half, t + 2), from_far.at[layer, s, half], 2 + layer, key, ways(s)[0])

    def sum_short(layer, s, half):
        _, _, way, near = ways(s)
        key = ("own", layer, s, half)
        send("z", block(layer, s, half, near), from_short.at[layer, s, half], 2 + layer, key, way)

    def sum_long(layer, s, half):
        need("z", ("far", layer, s, half), from_far.at[layer, s, half])
        way, near, _, _ = ways(s)
        mine = block(layer, s, half, near)
        came = from_far[layer, s, half].astype(jnp.float32)
        mine[...] = (mine[...].astype(jnp.float32) + came).astype(jnp.bfloat16)
        send("z", mine, from_long.at[layer, s, half], 2 + layer, ("own", layer, s, half), way)

    def sum_own(layer, s, half):
        need("z", ("own", layer, s, half), part.at[layer, s, pl.ds(0, 2 * H)])
        total = (
            block(layer, s, half, t)[...].astype(jnp.float32)
            + from_short[layer, s, half].astype(jnp.float32)
            + from_long[layer, s, half].astype(jnp.float32)
        )
        for k, chip in enumerate(SETS[s]):
            at = pl.ds(pl.multiple_of(owner(chip, 0) * (TILE // 2), TILE), TILE)
            branch[pl.ds(half * H, H), at] = total[:, k * TILE : (k + 1) * TILE]

    def norm(half):
        load_wait(*loads[:2])
        at = pl.ds(half * H, H)
        own_rows(0, half)[...] = rms_scale(tokens[at].astype(jnp.float32), early_norm[...]).astype(jnp.bfloat16)

    def start_mixed():
        load_wait(*loads)
        base[...] = tokens[...].astype(jnp.float32) + rms_scale(mixer[...].astype(jnp.float32), mixer_gain[...])

    def finish(layer, half):
        at = pl.ds(half * H, H)
        if layer == 0:
            keep = (base[at] + 0.5 * rms_scale(branch[at], early_post[...])).astype(jnp.bfloat16)
            mixed[at] = keep
            own_rows(1, half)[...] = rms_scale(keep.astype(jnp.float32), later_norm[...]).astype(jnp.bfloat16)
        else:
            out[at] = (
                mixed[at].astype(jnp.float32) + 0.5 * rms_scale(branch[at], later_post[...])
            ).astype(jnp.bfloat16)

    actions = {
        GATE0: lambda a, b: gate(0, None, a, b), VALUE0: lambda a, b: value(0, None, a, b),
        EARLY0: lambda a, b: value_early(0, None, a, b), EARLY1: lambda h, a, b: value_early(1, h, a, b),
        GATE1: lambda h, a, b: gate(1, h, a, b), VALUE1: lambda h, a, b: value(1, h, a, b),
        DOWN0: lambda s: down(0, s, None), DOWN1: lambda s, h: down(1, s, h),
        S2: sum_far, SS: sum_short, ADD: sum_long, OWN: sum_own, FIN: finish, BASE: start_mixed, NORM: norm,
        G1Z: functools.partial(gather, 1, "z+"), G1ZM: functools.partial(gather, 1, "z-"),
        G2Z: functools.partial(gather, 2, "z+"), G2ZM: functools.partial(gather, 2, "z-"),
        G3Z: functools.partial(gather, 3, "z+"), G3ZM: functools.partial(gather, 3, "z-"),
    }
    for kind in STEPS:
        actions[kind] = functools.partial(weights, kind)
    for kind, *numbers in ORDER:
        actions[kind](*numbers)

    for m in range(MATRICES):
        pltpu.make_async_copy(some(m, SENT), some(m, SENT), w_send.at[m]).wait()
    for layer in range(2):
        sent = all_rows[layer].at[pl.ds(0, 12 * U)]
        pltpu.make_async_copy(sent, sent, z_send.at[layer]).wait()
        sent = part.at[layer, pl.ds(0, 3)]
        pltpu.make_async_copy(sent, sent, z_send.at[2 + layer]).wait()


def on_device(*args):
    (tokens, mixer, early_norm, eg, ev, ed, early_post, mixer_gain, later_norm, lg, lv, ld, later_post) = args
    n, D = tokens.shape
    depth, wide = eg.shape
    F = D // depth
    H = n // 2
    bf16, f32 = jnp.bfloat16, jnp.float32
    gains = [x.reshape(1, D) for x in (early_norm, early_post, mixer_gain, later_norm, later_post)]
    vmem = pl.BlockSpec(memory_space=pltpu.VMEM)
    hbm = pl.BlockSpec(memory_space=pl.ANY)
    gathered = [pltpu.VMEM((F * depth, wide), bf16)] * 2 + [pltpu.VMEM((F,) + ed.shape, bf16)]
    landing = pltpu.VMEM((2, len(SETS), 2, H, 2 * TILE), bf16)
    w_count = MATRICES * len(ARRIVALS) + 6 + 2 * len(SETS)
    z_count = 2 * 2 * (3 + 2 * len(SETS))
    return pl.pallas_call(
        kernel,
        out_shape=pltpu.VMEM((n, D), bf16),
        in_specs=[hbm] * len(args),
        out_specs=vmem,
        scratch_shapes=[pltpu.VMEM((n, D), bf16)] * 2
        + [pltpu.VMEM((1, D), f32)] * 5
        + gathered * 2
        + [
            pltpu.VMEM((T * n, D), bf16),
            pltpu.VMEM((T * n, D), bf16),
            pltpu.VMEM((T * n, wide), f32),
            pltpu.VMEM((T * n, wide), f32),
            pltpu.VMEM((T * n, wide), bf16),
            pltpu.VMEM((2, len(SETS), T * n, 2 * TILE), bf16),
            pltpu.VMEM((n, D), f32),
            pltpu.VMEM((n, D), f32),
            pltpu.VMEM((n, D), bf16),
            landing,
            landing,
            landing,
            pltpu.SemaphoreType.DMA((MATRICES,)),
            pltpu.SemaphoreType.DMA((w_count,)),
            pltpu.SemaphoreType.DMA((MATRICES + 7,)),
            pltpu.SemaphoreType.DMA((4,)),
            pltpu.SemaphoreType.DMA((z_count,)),
        ],
        compiler_params=pltpu.CompilerParams(
            collective_id=0, has_side_effects=True, vmem_limit_bytes=66_000_000
        ),
    )(tokens, mixer, gains[0], eg, ev, ed, gains[1], gains[2], gains[3], lg, lv, ld, gains[4])


def solution(mesh):
    assert dict(mesh.shape) == {"rep": 2, "fs": 16, "tp": 4}
    rows = P(("rep", "fs", "tp"), None)
    up, down = P("fs", "tp"), P("tp", "fs")
    placed = (rows, rows, P(), up, up, down, P(), P(), P(), up, up, down, P())
    return jax.shard_map(on_device, mesh=mesh, in_specs=placed, out_specs=rows, check_vma=False)
```

```python
import functools

import jax
import jax.numpy as jnp
from jax import lax
from jax.experimental import pallas as pl
from jax.experimental.pallas import tpu as pltpu
from jax.sharding import PartitionSpec as P

epsilon = 1e-06
TILE = 256
Y, X, T = 4, 4, 4
MATRICES = 6

(
    OY1, OY2, OY3, OX1, OX2, F1, F2, X1, X3, QQ, E1, E2, OM, A2, A3, B2, C2, D1, D2, D3, D4, G1Z, G1ZM, G2Z,
    G2ZM, G3Z, G3ZM, S2, SS, ADD, OWN, FIN, GATE0, VALUE0, DOWN0, GATE1, VALUE1, DOWN1, BASE, EARLY0,
    EARLY1, NORM,
) = range(42)

ORDER = (
    (OY1, 0), (OM, 0), (OX1, 0), (OY2, 0), (OX2, 0), (NORM, 0), (G1Z, 0, 0), (G1ZM, 0, 0), (NORM, 1),
    (G1Z, 0, 1), (G1ZM, 0, 1), (BASE,), (OY3, 0), (OX1, 1), (G2Z, 0, 1), (G2ZM, 0, 1), (OX2, 1), (A2, 0),
    (F2, 0), (B2, 0), (OX1, 2), (G2Z, 0, 0), (G2ZM, 0, 0), (F1, 0), (X1, 0), (G3Z, 0, 1), (G3ZM, 0, 1), (A3, 0),
    (QQ, 0), (B2, 1), (X3, 0), (OY1, 1), (OM, 1), (G3Z, 0, 0), (G3ZM, 0, 0), (C2, 0), (OY2, 1), (D1, 0),
    (E2, 0), (D2, 0), (OY3, 1), (E1, 0), (D3, 0), (OX2, 2), (A2, 1), (F1, 1), (X1, 1), (QQ, 1), (D4, 0),
    (OX1, 3), (GATE0, 0, 1), (A3, 1), (B2, 2), (F2, 1), (X3, 1), (GATE0, 1, 3), (D1, 1), (OY1, 2), (OM, 2),
    (GATE0, 3, 5), (D2, 1), (OY2, 2), (E1, 1), (C2, 1), (OY3, 2), (E2, 1), (EARLY0, 0, 1), (D3, 1), (OX2, 3),
    (EARLY0, 1, 4), (A2, 2), (X1, 2), (F2, 2), (EARLY0, 4, 5), (F1, 2), (D4, 1), (OX1, 4), (VALUE0, 0, 1),
    (A3, 2), (B2, 3), (X3, 2), (OY1, 3), (OM, 3), (VALUE0, 1, 4), (D1, 2), (OY2, 3), (VALUE0, 4, 5), (DOWN0, 0),
    (SS, 0, 0, 1), (SS, 0, 0, 0), (S2, 0, 0, 1), (S2, 0, 0, 0), (DOWN0, 1), (C2, 2), (E2, 2), (S2, 0, 1, 0),
    (SS, 0, 1, 1), (QQ, 2), (S2, 0, 1, 1), (SS, 0, 1, 0), (F1, 3), (E1, 2), (ADD, 0, 0, 1), (A2, 3), (OY3, 3),
    (D3, 2), (X1, 3), (ADD, 0, 0, 0), (D2, 2), (OX2, 4), (ADD, 0, 1, 0), (DOWN0, 2), (D4, 2), (ADD, 0, 1, 1),
    (SS, 0, 2, 0), (S2, 0, 2, 0), (S2, 0, 2, 1), (SS, 0, 2, 1), (F2, 3), (E1, 3), (OWN, 0, 0, 1), (D1, 3),
    (QQ, 3), (OX1, 5), (DOWN0, 3), (S2, 0, 3, 0), (SS, 0, 3, 1), (SS, 0, 3, 0), (OWN, 0, 1, 0), (S2, 0, 3, 1),
    (OWN, 0, 0, 0), (A3, 3), (OY1, 4), (OM, 4), (B2, 4), (X3, 3), (OWN, 0, 1, 1), (ADD, 0, 2, 0), (C2, 3),
    (QQ, 4), (ADD, 0, 2, 1), (D2, 3), (OY2, 4), (E2, 3), (ADD, 0, 3, 0), (OY3, 4), (OX2, 5), (ADD, 0, 3, 1),
    (OWN, 0, 2, 0), (D2, 4), (D3, 3), (OWN, 0, 2, 1), (OWN, 0, 3, 0), (FIN, 0, 0), (G1Z, 1, 0), (G1ZM, 1, 0),
    (G2ZM, 1, 0), (G2Z, 1, 0), (A2, 4), (X1, 4), (D4, 3), (F1, 4), (OWN, 0, 3, 1), (FIN, 0, 1), (F2, 4),
    (B2, 5), (A3, 4), (X3, 4), (OY1, 5), (OM, 5), (D1, 4), (G3Z, 1, 0), (G3ZM, 1, 0), (OY2, 5), (G1Z, 1, 1),
    (G1ZM, 1, 1), (E1, 4), (C2, 4), (OY3, 5), (E2, 4), (G2Z, 1, 1), (G2ZM, 1, 1), (D3, 4), (GATE1, 0, 0, 1),
    (A2, 5), (X1, 5), (F1, 5), (GATE1, 0, 1, 5), (F2, 5), (EARLY1, 0, 0, 1), (D4, 4), (EARLY1, 0, 1, 3),
    (G3ZM, 1, 1), (G3Z, 1, 1), (EARLY1, 0, 3, 5), (A3, 5), (X3, 5), (QQ, 5), (D1, 5), (VALUE1, 0, 0, 5),
    (DOWN1, 0, 0), (SS, 1, 0, 0), (S2, 1, 0, 0), (E1, 5), (DOWN1, 1, 0), (SS, 1, 1, 0), (S2, 1, 1, 0), (C2, 5),
    (E2, 5), (GATE1, 1, 0, 2), (D2, 5), (D3, 5), (GATE1, 1, 2, 4), (ADD, 1, 0, 0), (GATE1, 1, 4, 5),
    (EARLY1, 1, 0, 3), (ADD, 1, 1, 0), (DOWN1, 2, 0), (SS, 1, 2, 0), (S2, 1, 2, 0), (EARLY1, 1, 3, 5),
    (VALUE1, 1, 0, 2), (D4, 5), (VALUE1, 1, 2, 5), (OWN, 1, 0, 0), (DOWN1, 0, 1), (SS, 1, 0, 1), (S2, 1, 0, 1),
    (DOWN1, 1, 1), (S2, 1, 1, 1), (SS, 1, 1, 1), (DOWN1, 2, 1), (SS, 1, 2, 1), (S2, 1, 2, 1), (OWN, 1, 1, 0),
    (DOWN1, 3, 0), (ADD, 1, 2, 0), (DOWN1, 3, 1), (S2, 1, 3, 0), (SS, 1, 3, 0), (S2, 1, 3, 1), (ADD, 1, 0, 1),
    (ADD, 1, 1, 1), (SS, 1, 3, 1), (ADD, 1, 2, 1), (OWN, 1, 2, 0), (ADD, 1, 3, 0), (ADD, 1, 3, 1),
    (OWN, 1, 0, 1), (OWN, 1, 1, 1), (OWN, 1, 3, 0), (FIN, 1, 0), (OWN, 1, 2, 1), (OWN, 1, 3, 1), (FIN, 1, 1),
)

SETS = (((0, 0), (3, 0)), ((1, 0), (0, 1)), ((2, 0), (3, 1)), ((1, 1), (2, 1)))
LATE = ((3, 1), (1, 1), (2, 1))
EARLY = tuple(chip for chips in SETS for chip in chips if chip not in LATE)
SET_OF = {chip: s for s, chips in enumerate(SETS) for chip in chips}
STEPS = {
    OY1: ((), (("y+", (0, 0), 0, 1), ("y-", (0, 0), 2, 1)), "W1"),
    OY2: ((), (("y+", (0, 0), 1, 1), ("y-", (0, 0), 3, 1)), "W2"),
    OY3: ((), (("y+", (0, 0), 2, 2), ("y-", (0, 0), 0, 2)), "W3"),
    OX1: ((), (("x+", (0, 0), 0, 1), ("x-", (0, 0), 2, 1)), "X1"),
    OX2: ((), (("x+", (0, 0), 1, 1), ("x-", (0, 0), 3, 1)), "X2"),
    F1: (("W1",), (("y+", (3, 0), 0, 1), ("y-", (1, 0), 2, 1)), "F1"),
    F2: (("W2",), (("y+", (3, 0), 1, 1), ("y-", (1, 0), 3, 1)), "F2"),
    X1: (("W2",), (("x+", (3, 0), 1, 1), ("x-", (1, 0), 3, 1)), "D1"),
    X3: (("W3",), (("x-", (3, 0), 2, 2), ("x+", (1, 0), 0, 2)), "D3"),
    QQ: (("X1",), (("y+", (0, 1), 0, 1), ("y-", (0, 1), 2, 1)), "D2"),
    E1: (("F1",), (("x+", (2, 0), 0, 1), ("x-", (2, 0), 2, 1)), "E1"),
    E2: (("F2",), (("x+", (2, 0), 1, 1), ("x-", (2, 0), 3, 1)), "E2"),
    OM: ((), (("mate", (0, 0), 0, 4),), None),
    A2: (("W1", "W2"), (("mate", (3, 0), 0, 2), ("mate", (1, 0), 2, 2)), None),
    A3: (("W3",), (("mate", (3, 0), 2, 2), ("mate", (1, 0), 0, 2)), None),
    B2: (("X1", "X2"), (("mate", (0, 1), 0, 4),), None),
    C2: (("F1", "F2"), (("mate", (2, 0), 0, 4),), None),
    D1: (("D1",), (("mate", (3, 1), 1, 1), ("mate", (1, 1), 3, 1)), None),
    D2: (("D2",), (("mate", (3, 1), 0, 1), ("mate", (1, 1), 2, 1)), None),
    D3: (("D3",), (("mate", (3, 1), 2, 2), ("mate", (1, 1), 0, 2)), None),
    D4: (("E1", "E2"), (("mate", (2, 1), 0, 4),), None),
}
ARRIVALS = {arrival: sum(c[3] for c in moves) for _, moves, arrival in STEPS.values() if arrival}
SENT = sum(c[3] for _, moves, _ in STEPS.values() for c in moves)


def rms_scale(values, gain):
    scale = lax.rsqrt(jnp.mean(values * values, axis=-1, keepdims=True) + epsilon)
    return values * scale * gain


def kernel(
    tokens_in, mixer_in, early_norm_in, w0, w1, w2, early_post_in, mixer_gain_in, later_norm_in, w3, w4, w5,
    later_post_in,
    out,
    tokens, mixer, early_norm, early_post, mixer_gain, later_norm, later_post,
    g0, g1, g2, g3, g4, g5, rows0, rows1, gate_sum, value_sum, hidden, part, base, branch, mixed, from_far, from_short, from_long,
    w_send, w_recv, local_sem, z_send, z_recv,
):
    source = (w0, w1, w2, w3, w4, w5)
    full = (g0, g1, g2, g3, g4, g5)
    all_rows = (rows0, rows1)
    r, f, t = lax.axis_index("rep"), lax.axis_index("fs"), lax.axis_index("tp")
    c = f % 2
    xl = f // 2 % 2
    y = f // 4
    x = r * 2 + xl
    n, D = tokens.shape
    H = n // 2
    M = T * H
    U = H // 2

    def chip(dx, dy):
        xx = (x + dx) % X
        return {"rep": xx // 2, "fs": ((y + dy) % Y * 2 + xx % 2) * 2 + c}

    where = {
        "y+": chip(0, 1), "y-": chip(0, Y - 1), "x+": chip(1, 0), "x-": chip(X - 1, 0),
        "mate": {"fs": f + 1 - 2 * c}, "z+": {"tp": (t + 1) % T}, "z-": {"tp": (t + T - 1) % T},
    }

    def owner(chip, core):
        dy, other = chip
        return ((y + dy) % Y * 2 + (xl + other) % 2) * 2 + core

    def piece(m, shard, first, quarters):
        quarter = source[m].shape[0] // 4
        if m % 3 == 2:
            return full[m].at[shard, pl.ds(first * quarter, quarters * quarter)]
        start = pl.multiple_of(shard * 4 * quarter + first * quarter, quarter)
        return full[m].at[pl.ds(start, quarters * quarter)]

    def some(m, quarters):
        if m % 3 == 2:
            if quarters % 4 == 0:
                return full[m].at[pl.ds(0, quarters // 4)]
            return full[m].at[0, pl.ds(0, quarters * (source[m].shape[0] // 4))]
        return full[m].at[pl.ds(0, quarters * (source[m].shape[0] // 4))]

    barrier = pltpu.get_barrier_semaphore()
    for who in where.values():
        pl.semaphore_signal(barrier, inc=1, device_id=who, device_id_type=pl.DeviceIdType.MESH)
    inputs = (
        (tokens_in, tokens), (early_norm_in, early_norm), (mixer_in, mixer), (mixer_gain_in, mixer_gain),
        (early_post_in, early_post), (later_norm_in, later_norm), (later_post_in, later_post),
    )
    loads = [pltpu.make_async_copy(*pair, local_sem.at[MATRICES + k]) for k, pair in enumerate(inputs)]
    local = [
        pltpu.make_async_copy(source[m], piece(m, f, 0, 4), local_sem.at[m]) for m in range(MATRICES)
    ]
    for load in local[:1] + loads + local[1:]:
        load.start()
    loaded = set()

    def load_wait(*copies):
        for copy in copies:
            if id(copy) not in loaded:
                loaded.add(id(copy))
                copy.wait()

    def own_rows(layer, half):
        return all_rows[layer].at[pl.ds(pl.multiple_of(half * M + t * H, H), H)]

    pl.semaphore_wait(barrier, len(where))

    slots = {"w": {}, "z": {}}
    arrived = set()

    def slot(kind, key):
        return slots[kind].setdefault(key, len(slots[kind]))

    def send(kind, src, dst, out_slot, key, way):
        sems = (w_send, w_recv) if kind == "w" else (z_send, z_recv)
        pltpu.make_async_remote_copy(
            src_ref=src, dst_ref=dst, send_sem=sems[0].at[out_slot], recv_sem=sems[1].at[slot(kind, key)],
            device_id=where[way], device_id_type=pl.DeviceIdType.MESH,
        ).start()

    def need(kind, key, same_bytes):
        if key not in arrived:
            arrived.add(key)
            sem = (w_recv if kind == "w" else z_recv).at[slot(kind, key)]
            pltpu.make_async_copy(same_bytes, same_bytes, sem).wait()

    def weights(name, m):
        waits, moves, arrival = STEPS[name]
        for key in waits:
            need("w", (key, m), some(m, ARRIVALS[key]))
        for way, chip, first, quarters in moves:
            if chip == (0, 0):
                load_wait(local[m])
            ref = piece(m, owner(chip, c), first, quarters)
            key = arrival or ("mate", (None, chip in LATE, SET_OF[chip])[m % 3])
            send("w", ref, ref, m, (key, m), way)

    def ready(m, s, shards):
        need("w", (("mate", s), m), some(m, 4 * shards))

    def row_piece(layer, half, block, u):
        start = pl.multiple_of(half * M + block % T * H + u * U, U)
        return all_rows[layer].at[pl.ds(start, U)]

    def gather(step, way, layer, half):
        u = (0 if way == "z+" else 1) if step != 2 else (1 if way == "z+" else 0)
        block = t
        if step == 3:
            gathered(1, layer, half)
            block = t + T - 1 if way == "z+" else t + 1
        ref = row_piece(layer, half, block, u)
        send("z", ref, ref, layer, ("rows", step, layer, half), way)

    def gathered(step, layer, half):
        need("z", ("rows", step, layer, half), all_rows[layer].at[pl.ds(0, 2 * U)])

    def all_gathered(layer, half):
        for step in (1, 2, 3):
            gathered(step, layer, half)

    def span(rows):
        return pl.ds(0, 2 * M) if rows is None else pl.ds(rows * M, M)

    def gate(layer, rows, first, last):
        weight = full[3 * layer]
        ready(3 * layer, None, 8)
        for half in range(2) if rows is None else (rows,):
            all_gathered(layer, half)

        @pl.loop(first, last)
        def _(j):
            at = pl.ds(pl.multiple_of(j * TILE, TILE), TILE)
            gate_sum[span(rows), at] = jnp.dot(
                all_rows[layer][span(rows)], weight[:, at], preferred_element_type=jnp.float32
            )

    def partial_dot(layer, rows, weight, chips, at):
        spots = [pl.ds(pl.multiple_of(owner(chip, 0) * 128, 256), 256) for chip in chips]
        left = jnp.concatenate([all_rows[layer][span(rows), spot] for spot in spots], axis=1)
        right = jnp.concatenate([weight[spot, at] for spot in spots], axis=0)
        return jnp.dot(left, right, preferred_element_type=jnp.float32)

    def value_early(layer, rows, first, last):
        weight = full[3 * layer + 1]
        ready(3 * layer + 1, False, len(EARLY))
        for half in range(2) if rows is None else (rows,):
            all_gathered(layer, half)

        @pl.loop(first, last)
        def _(j):
            at = pl.ds(pl.multiple_of(j * TILE, TILE), TILE)
            value_sum[span(rows), at] = partial_dot(layer, rows, weight, EARLY, at)

    def value(layer, rows, first, last):
        weight = full[3 * layer + 1]
        ready(3 * layer + 1, True, len(LATE))

        @pl.loop(first, last)
        def _(j):
            at = pl.ds(pl.multiple_of(j * TILE, TILE), TILE)
            b = value_sum[span(rows), at] + partial_dot(layer, rows, weight, LATE, at)
            a = gate_sum[span(rows), at]
            hidden[span(rows), at] = (a / (1.0 + jnp.exp(-a)) * b).astype(jnp.bfloat16)

    def down(layer, s, rows):
        weight = full[3 * layer + 2]
        ready(3 * layer + 2, s, 2)
        for k, chip in enumerate(SETS[s]):
            both = jnp.concatenate([weight[owner(chip, 0)], weight[owner(chip, 1)]], axis=1)
            sums = jnp.dot(hidden[span(rows)], both, preferred_element_type=jnp.float32)
            part[layer, s, span(rows), pl.ds(k * TILE, TILE)] = sums.astype(jnp.bfloat16)

    def block(layer, s, half, b):
        return part.at[layer, s, pl.ds(pl.multiple_of(half * M + b % T * H, H), H)]

    def ways(s):
        right, left = ("z+", t + 1), ("z-", t + T - 1)
        return right + left if s % 2 == 0 else left + right

    def sum_far(layer, s, half):
        key = ("far", layer, s, half)
        send("z", block(layer, s, half, t + 2), from_far.at[layer, s, half], 2 + layer, key, ways(s)[0])

    def sum_short(layer, s, half):
        _, _, way, near = ways(s)
        key = ("own", layer, s, half)
        send("z", block(layer, s, half, near), from_short.at[layer, s, half], 2 + layer, key, way)

    def sum_long(layer, s, half):
        need("z", ("far", layer, s, half), from_far.at[layer, s, half])
        way, near, _, _ = ways(s)
        mine = block(layer, s, half, near)
        came = from_far[layer, s, half].astype(jnp.float32)
        mine[...] = (mine[...].astype(jnp.float32) + came).astype(jnp.bfloat16)
        send("z", mine, from_long.at[layer, s, half], 2 + layer, ("own", layer, s, half), way)

    def sum_own(layer, s, half):
        need("z", ("own", layer, s, half), part.at[layer, s, pl.ds(0, 2 * H)])
        total = (
            block(layer, s, half, t)[...].astype(jnp.float32)
            + from_short[layer, s, half].astype(jnp.float32)
            + from_long[layer, s, half].astype(jnp.float32)
        )
        for k, chip in enumerate(SETS[s]):
            at = pl.ds(pl.multiple_of(owner(chip, 0) * (TILE // 2), TILE), TILE)
            branch[pl.ds(half * H, H), at] = total[:, k * TILE : (k + 1) * TILE]

    def norm(half):
        load_wait(*loads[:2])
        at = pl.ds(half * H, H)
        own_rows(0, half)[...] = rms_scale(tokens[at].astype(jnp.float32), early_norm[...]).astype(jnp.bfloat16)

    def start_mixed():
        load_wait(*loads)
        base[...] = tokens[...].astype(jnp.float32) + rms_scale(mixer[...].astype(jnp.float32), mixer_gain[...])

    def finish(layer, half):
        at = pl.ds(half * H, H)
        if layer == 0:
            keep = (base[at] + 0.5 * rms_scale(branch[at], early_post[...])).astype(jnp.bfloat16)
            mixed[at] = keep
            own_rows(1, half)[...] = rms_scale(keep.astype(jnp.float32), later_norm[...]).astype(jnp.bfloat16)
        else:
            out[at] = (
                mixed[at].astype(jnp.float32) + 0.5 * rms_scale(branch[at], later_post[...])
            ).astype(jnp.bfloat16)

    actions = {
        GATE0: lambda a, b: gate(0, None, a, b), VALUE0: lambda a, b: value(0, None, a, b),
        EARLY0: lambda a, b: value_early(0, None, a, b), EARLY1: lambda h, a, b: value_early(1, h, a, b),
        GATE1: lambda h, a, b: gate(1, h, a, b), VALUE1: lambda h, a, b: value(1, h, a, b),
        DOWN0: lambda s: down(0, s, None), DOWN1: lambda s, h: down(1, s, h),
        S2: sum_far, SS: sum_short, ADD: sum_long, OWN: sum_own, FIN: finish, BASE: start_mixed, NORM: norm,
        G1Z: functools.partial(gather, 1, "z+"), G1ZM: functools.partial(gather, 1, "z-"),
        G2Z: functools.partial(gather, 2, "z+"), G2ZM: functools.partial(gather, 2, "z-"),
        G3Z: functools.partial(gather, 3, "z+"), G3ZM: functools.partial(gather, 3, "z-"),
    }
    for kind in STEPS:
        actions[kind] = functools.partial(weights, kind)
    for kind, *numbers in ORDER:
        actions[kind](*numbers)

    for m in range(MATRICES):
        pltpu.make_async_copy(some(m, SENT), some(m, SENT), w_send.at[m]).wait()
    for layer in range(2):
        sent = all_rows[layer].at[pl.ds(0, 12 * U)]
        pltpu.make_async_copy(sent, sent, z_send.at[layer]).wait()
        sent = part.at[layer, pl.ds(0, 3)]
        pltpu.make_async_copy(sent, sent, z_send.at[2 + layer]).wait()


def on_device(*args):
    (tokens, mixer, early_norm, eg, ev, ed, early_post, mixer_gain, later_norm, lg, lv, ld, later_post) = args
    n, D = tokens.shape
    depth, wide = eg.shape
    F = D // depth
    H = n // 2
    bf16, f32 = jnp.bfloat16, jnp.float32
    gains = [x.reshape(1, D) for x in (early_norm, early_post, mixer_gain, later_norm, later_post)]
    vmem = pl.BlockSpec(memory_space=pltpu.VMEM)
    hbm = pl.BlockSpec(memory_space=pl.ANY)
    gathered = [pltpu.VMEM((F * depth, wide), bf16)] * 2 + [pltpu.VMEM((F,) + ed.shape, bf16)]
    landing = pltpu.VMEM((2, len(SETS), 2, H, 2 * TILE), bf16)
    w_count = MATRICES * len(ARRIVALS) + 6 + 2 * len(SETS)
    z_count = 2 * 2 * (3 + 2 * len(SETS))
    return pl.pallas_call(
        kernel,
        out_shape=pltpu.VMEM((n, D), bf16),
        in_specs=[hbm] * len(args),
        out_specs=vmem,
        scratch_shapes=[pltpu.VMEM((n, D), bf16)] * 2
        + [pltpu.VMEM((1, D), f32)] * 5
        + gathered * 2
        + [
            pltpu.VMEM((T * n, D), bf16),
            pltpu.VMEM((T * n, D), bf16),
            pltpu.VMEM((T * n, wide), f32),
            pltpu.VMEM((T * n, wide), f32),
            pltpu.VMEM((T * n, wide), bf16),
            pltpu.VMEM((2, len(SETS), T * n, 2 * TILE), bf16),
            pltpu.VMEM((n, D), f32),
            pltpu.VMEM((n, D), f32),
            pltpu.VMEM((n, D), bf16),
            landing,
            landing,
            landing,
            pltpu.SemaphoreType.DMA((MATRICES,)),
            pltpu.SemaphoreType.DMA((w_count,)),
            pltpu.SemaphoreType.DMA((MATRICES + 7,)),
            pltpu.SemaphoreType.DMA((4,)),
            pltpu.SemaphoreType.DMA((z_count,)),
        ],
        compiler_params=pltpu.CompilerParams(
            collective_id=0, has_side_effects=True, vmem_limit_bytes=66_000_000
        ),
    )(tokens, mixer, gains[0], eg, ev, ed, gains[1], gains[2], gains[3], lg, lv, ld, gains[4])


def solution(mesh):
    assert dict(mesh.shape) == {"rep": 2, "fs": 16, "tp": 4}
    rows = P(("rep", "fs", "tp"), None)
    up, down = P("fs", "tp"), P("tp", "fs")
    placed = (rows, rows, P(), up, up, down, P(), P(), P(), up, up, down, P())
    return jax.shard_map(on_device, mesh=mesh, in_specs=placed, out_specs=rows, check_vma=False)
```
